128 devices in a mesh: sp: 16 (over z, x), tp: 8 (over y, core).
Axes of the slice: x: 4, y: 4, z: 4, core: 2. Of those that a mesh axis runs over, the one named last changes fastest.
Arguments:
- stream: bfloat16 [4096, 2048], P(('sp', 'tp')), may hold values from -5 to 5
- out_gate: bfloat16 [4096, 2048], P('sp', 'tp'), may hold values from -6 to 6
- in_gate: bfloat16 [4096, 2048], P('sp', 'tp'), may hold values from -6 to 6
- values: bfloat16 [4096, 2048], P('sp', 'tp'), may hold values from -6 to 6
- conv_weight: float32 [3, 2048], P(None, 'tp'), may hold values from -3 to 3
- out_weight: bfloat16 [2048, 2048], replicated, may hold values from -0.125 to 0.125
- doc_ids: int32 [4096], P('sp'), may hold values from 0 to 5, never falling along the last dimension, each value on 1 to 1024 neighbouring positions
- routes: int32 [4096, 2], P(('sp', 'tp')), may hold values from 0 to 15, all different within a row; in each aligned block of 32 rows (0 to 31, 32 to 63, ...) at most 5 rows name the same one
- route_weight: float32 [4096, 2], P(('sp', 'tp')), may hold values from 0.2 to 1
- norm_gain: float32 [2, 2048], replicated, may hold values from 0.1 to 1.9
- norm_bias: float32 [2, 2048], replicated, may hold values from -2 to 2
- expert_gate: bfloat16 [16, 2048, 7168], P('sp', None, 'tp'), may hold values from -0.125 to 0.125
- expert_up: bfloat16 [16, 2048, 7168], P('sp', None, 'tp'), may hold values from -0.125 to 0.125
- expert_down: bfloat16 [16, 7168, 2048], P('sp', 'tp'), may hold values from -0.0625 to 0.0625
Outputs:
- layer_out: bfloat16 [4096, 2048], P(('sp', 'tp'))
The draws below stay inside these ranges and needn't reach their ends.
Inputs may be any that keep to these rules, and one draw needn't show every extreme that they name: `doc_ids`: each document occupies consecutive positions, numbers never fall along positions, each document has at most 1024 positions and one has exactly 1024. `routes`: each row names two different experts. In each aligned block of 32 rows (the rows of one device) no expert is named more than 5 times, a bound that some block reaches.
All inputs are finite; a program needn't handle non-finite values.
Results may differ from the reference program's by a relative error of at most 0.012.
Values may be sent and summed in bfloat16 or wider, within the bound.
A program may use at most 64 MiB of HBM per device.

```python
import math
import jax
import jax.numpy as jnp
import numpy as np
from jax import lax

D = 2048
FF = 7168
TOK_DEV = 256
TOKENS = 4096
EXPERTS = 16
CAP = 5
DOCS = 6
DOC_MOST = 1024
N_SP = 16
N_TP = 8


def levels(rng, dims, cuts, smallest, largest):
    def one(position, blocks):
        heights = jax.random.uniform(jax.random.fold_in(jax.random.fold_in(rng, 6), position), (blocks,), jnp.float32, smallest / len(cuts), largest / len(cuts))
        return jnp.repeat(jnp.exp(heights), dims[position] // blocks).reshape((-1,) + (1,) * (len(dims) - position - 1))

    level = one(*cuts[0])
    for cut in cuts[1:]:
        level = level * one(*cut)
    return level


def profile(number_of, total, limit, lean):
    portions = [(1 << 20) // math.isqrt(standing ** lean) + 1 for standing in range(2, number_of + 1)]
    rest, counts = total - limit - (number_of - 1), [1] * (number_of - 1)
    while rest > 0:
        candidates = [i for i in range(number_of - 1) if counts[i] < limit]
        mass, budget = sum([portions[i] for i in candidates]), rest
        for i in candidates:
            addition = min(limit - counts[i], max(1, budget * portions[i] // mass), rest)
            counts[i] = counts[i] + addition
            rest = rest - addition
    return np.array([limit] + counts)


def ragged(stream_key, amount, total, limit, slope):
    if amount == 2:
        one = jax.random.randint(stream_key, (), max(1, total - limit), min(limit, total - 1) + 1)
        return jnp.stack([one, total - one])
    sizes = jnp.asarray(profile(amount, total, limit, slope), jnp.int32)
    couples = (amount - 1) // 2
    donor, receiver = sizes[1:1 + 2 * couples:2], sizes[2:2 + 2 * couples:2]
    margin = jnp.minimum(donor - 1, limit - receiver)
    passed = jax.random.randint(jax.random.fold_in(stream_key, 1), (couples,), 0, 1 << 20) % (margin + 1)
    sizes = sizes.at[1:1 + 2 * couples:2].set(donor - passed).at[2:2 + 2 * couples:2].set(receiver + passed)
    return sizes[jax.random.permutation(jax.random.fold_in(stream_key, 2), amount)]


def routed_block(rng, own, number, rows, number_of, top, bound, lean):
    ranking = jax.random.permutation(rng, number_of)
    crowded, usual = shares(number_of, rows * top, bound, lean, True), shares(number_of, rows * top, bound, lean, False)
    places = jnp.arange(number_of)

    def named(sizes, turn):
        used = int((sizes > 0).sum())
        fixed = max(1, used // 4)
        shifted = fixed + (places - fixed + turn * (used - fixed)) % max(1, number_of - fixed)
        return jnp.zeros((number_of,), jnp.int32).at[ranking[jnp.where(places < fixed, places, shifted)]].set(jnp.asarray(sizes, jnp.int32))

    sizes = jnp.where(number % 4 == 0, named(crowded, number // 4), named(usual, number - number // 4 - 1))
    mixed = jax.random.permutation(jax.random.fold_in(own, 3), number_of)
    giver, sink = mixed[0:number_of // 2 * 2:2], mixed[1:number_of // 2 * 2:2]
    margin = jnp.minimum(sizes[giver] - 1, bound - sizes[sink]) // 2
    margin = jnp.where((giver == ranking[0]) | (sink == ranking[0]) | (sizes[sink] == 0), 0, jnp.maximum(margin, 0))
    shifted = jax.random.randint(jax.random.fold_in(own, 4), (number_of // 2,), 0, 1 << 20) % (margin + 1)
    sizes = sizes.at[giver].add(-shifted).at[sink].add(shifted)
    items = jnp.searchsorted(jnp.cumsum(sizes), jnp.arange(rows * top), side="right").astype(jnp.int32)
    listing = items.reshape(top, rows).T
    listing = listing[jax.random.permutation(jax.random.fold_in(own, 1), rows)]
    turn = jax.random.randint(jax.random.fold_in(own, 2), (rows, 1), 0, top)
    return jnp.take_along_axis(listing, (jnp.arange(top)[None, :] + turn) % top, axis=1)


def shares(amount, total, bound, skew, full):
    portions = [(1 << 20) // math.isqrt(standing ** skew) + 1 for standing in range(1, amount + 1)]
    largest = bound if full else min(bound, max(-(-total // amount), total * portions[0] // sum(portions)))
    least = 1 if total - largest >= amount - 1 else 0
    holding, spare = [largest] + [least] * (amount - 1), total - largest - least * (amount - 1)
    while spare > 0:
        candidates = [i for i in range(1, amount) if holding[i] < largest] or [i for i in range(1, amount) if holding[i] < bound]
        mass, left = sum([portions[i] for i in candidates]), spare
        for i in candidates:
            extra = min(bound - holding[i], max(1, left * portions[i] // mass), spare)
            holding[i] = holding[i] + extra
            spare = spare - extra
    return np.array(holding)


def noise(rng, extent, scale, bound, pieces=(), kind=jnp.bfloat16):
    values = jax.random.normal(rng, extent, jnp.float32) * scale
    if len(pieces) > 0:
        values = levels(rng, extent, pieces, -0.22, 0.18) * values
    return jnp.clip(values, min=-bound, max=bound).astype(kind)


def setup_inputs(seed: int = 0) -> dict:
    key_of = jax.random.split(jax.random.key(seed), 15)
    stream = noise(key_of[0], (TOKENS, D), 0.6, 5.0, ((0, 128),))
    out_gate = noise(key_of[1], (TOKENS, D), 1.0, 6.0, ((0, 16), (1, 8)))
    in_gate = noise(key_of[2], (TOKENS, D), 1.0, 6.0, ((0, 16), (1, 8)))
    values = noise(key_of[3], (TOKENS, D), 1.0, 6.0, ((0, 16), (1, 8)))
    conv_weight = noise(key_of[4], (3, D), 0.577, 3.0, ((1, 8),), jnp.float32)
    out_weight = noise(key_of[5], (D, D), D ** -0.5, 0.125)
    doc_ids = jnp.searchsorted(jnp.cumsum(ragged(key_of[6], DOCS, TOKENS, DOC_MOST, 1)), jnp.arange(TOKENS), side="right").astype(jnp.int32)
    routes_keys = jax.random.split(jax.random.fold_in(key_of[7], 1), TOKENS // (TOK_DEV // N_TP))
    routes_turns = jax.random.permutation(jax.random.fold_in(key_of[7], 3), TOKENS // (TOK_DEV // N_TP))
    routes = jax.vmap(lambda own, number: routed_block(jax.random.fold_in(key_of[7], 2), own, number, TOK_DEV // N_TP, EXPERTS, 2, CAP, 1))(routes_keys, routes_turns).reshape((TOKENS, 2))
    route_weight = jnp.clip(0.2 + 0.8 * jax.random.uniform(key_of[8], (TOKENS, 2), jnp.float32) ** levels(key_of[8], (TOKENS, 2), ((0, 128),), -0.2, 0.2), 0.2, 1.0)
    norm_gain = jnp.clip(1.0 + 0.18 * jax.random.normal(key_of[9], (2, D), jnp.float32), 0.1, 1.9)
    norm_bias = noise(key_of[10], (2, D), 0.3, 2.0, (), jnp.float32)
    expert_gate = noise(key_of[11], (EXPERTS, D, FF), D ** -0.5, 0.125, ((0, 16), (2, 8)))
    expert_up = noise(key_of[12], (EXPERTS, D, FF), D ** -0.5, 0.125, ((0, 16), (2, 8)))
    expert_down = noise(key_of[13], (EXPERTS, FF, D), FF ** -0.5, 0.0625, ((0, 16), (1, 8)))
    return {"stream": stream, "out_gate": out_gate, "in_gate": in_gate, "values": values, "conv_weight": conv_weight, "out_weight": out_weight, "doc_ids": doc_ids, "routes": routes, "route_weight": route_weight, "norm_gain": norm_gain, "norm_bias": norm_bias, "expert_gate": expert_gate, "expert_up": expert_up, "expert_down": expert_down}


residual_scale = 1.6817928

def layer_norm(values_in, gain_row, bias_row):
    row_mean = lax.optimization_barrier(jnp.mean(values_in, axis=-1, keepdims=True))
    centered = values_in - row_mean
    variance = lax.optimization_barrier(jnp.mean(centered * centered, axis=-1, keepdims=True))
    return centered * lax.rsqrt(variance + 1e-05) * gain_row + bias_row

def reference(stream, out_gate, in_gate, values, conv_weight, out_weight, doc_ids, routes, route_weight, norm_gain, norm_bias, expert_gate, expert_up, expert_down):
    length = doc_ids.shape[0]
    gated_values = in_gate.astype(jnp.float32) * values.astype(jnp.float32)
    extended = jnp.pad(gated_values, ((2, 0), (0, 0)))
    ext_docs = jnp.concatenate([jnp.full((2,), -1, jnp.int32), doc_ids])
    keep_first = (ext_docs[1:length + 1] == doc_ids).astype(jnp.float32)[:, None]
    keep_second = (ext_docs[0:length] == doc_ids).astype(jnp.float32)[:, None]
    convolved = conv_weight[0] * extended[0:length] * keep_second + conv_weight[1] * extended[1:length + 1] * keep_first + conv_weight[2] * gated_values
    mixed_rows = (out_gate.astype(jnp.float32) * convolved).astype(jnp.bfloat16)
    projected = jnp.dot(mixed_rows, out_weight, preferred_element_type=jnp.float32)
    normed = layer_norm(residual_scale * stream.astype(jnp.float32) + projected, norm_gain[0], norm_bias[0]).astype(jnp.bfloat16)
    block_rows = TOK_DEV // N_TP
    sources = N_SP * N_TP
    expert_ids = routes.reshape(sources, 2 * block_rows)
    onehot = (expert_ids[:, :, None] == jnp.arange(EXPERTS, dtype=jnp.int32)[None, None, :]).astype(jnp.int32)
    slot_rank = lax.optimization_barrier(jnp.sum((jnp.cumsum(onehot, axis=1) - onehot) * onehot, axis=-1)).astype(jnp.int32)
    source_ids = jnp.arange(sources, dtype=jnp.int32)[:, None]
    dest_rows = (source_ids * CAP + slot_rank).reshape(-1).astype(jnp.int32)
    expert_flat = expert_ids.reshape(-1).astype(jnp.int32)
    repeated = jnp.repeat(normed, 2, axis=0)
    buffer = jnp.zeros((EXPERTS, sources * CAP, D), jnp.bfloat16).at[expert_flat, dest_rows].set(repeated)
    part_width = FF // N_TP

    def expert(expert_item):
        rows, gate_w, up_w, down_w = expert_item
        gate_part = jnp.dot(rows, gate_w, preferred_element_type=jnp.float32)
        up_part = jnp.dot(rows, up_w, preferred_element_type=jnp.float32)
        hidden = (jax.nn.silu(gate_part) * up_part).astype(jnp.bfloat16)
        accumulated = jnp.zeros((rows.shape[0], D), jnp.float32)
        for shard in range(N_TP):
            partial_value = jnp.dot(hidden[:, shard * part_width:(shard + 1) * part_width], down_w[shard * part_width:(shard + 1) * part_width], preferred_element_type=jnp.float32).astype(jnp.bfloat16)
            partial_value = lax.optimization_barrier(partial_value)
            accumulated = accumulated + partial_value.astype(jnp.float32)
        return accumulated.astype(jnp.bfloat16)
    outputs = lax.map(expert, (buffer, expert_gate, expert_up, expert_down))
    picked = outputs[expert_flat, dest_rows].astype(jnp.float32).reshape(length, 2, D)
    routed_sum = lax.optimization_barrier(jnp.sum(picked * route_weight[:, :, None], axis=1))
    return layer_norm(residual_scale * normed.astype(jnp.float32) + routed_sum, norm_gain[1], norm_bias[1]).astype(jnp.bfloat16)
```

```python
import jax
import jax.numpy as jnp
from jax import lax
from jax.experimental import pallas as pl
from jax.experimental.pallas import tpu as pltpu
from jax.sharding import PartitionSpec as P

MESH = pl.DeviceIdType.MESH
RESIDUAL = 1.6817928
NX = 4
NZ = 4
NSP = 16
NTP = 8
CAP = 5
PAD = 8
NT = 4
F32 = jnp.float32
BF16 = jnp.bfloat16


def layer_norm(v, gain, bias):
    mean = jnp.mean(v, axis=-1, keepdims=True)
    cent = v - mean
    var = jnp.mean(cent * cent, axis=-1, keepdims=True)
    return cent * lax.rsqrt(var + 1e-05) * gain + bias


def one_hot(cond):
    return jnp.where(cond, 1.0, 0.0).astype(BF16)


def body(
    stream_h, og_h, ig_h, va_h, cw_h, ow_h, doc_h, rt_h, rw_h, ng_h, nb_h, wg_h, wu_h, wd_h,
    out_ref,
    stream, og, ig, va, cw, ow, doc, rt, rw, ng, nb, wg, wu, wd,
    ext, halo, mx, tr, acc, normed, snd, rcv, xb, hb, pf, pb, rd, q3, q1, q2, tq, ra, rb, snd2, ret,
    lsem, h_s, h_r, a_s, a_r, b_s, b_r, g_s, g_r, p_s, p_r, d_s, d_r, s3_s, s3_r, s2_s, s2_r, s1_s, s1_r, e_s, e_r,
):
    sp = lax.axis_index("sp")
    tp = lax.axis_index("tp")
    z, x = sp // NX, sp % NX
    y, c = tp // 2, tp % 2
    width = og.shape[1]
    length = og.shape[0]
    model = stream.shape[1]
    rows = stream.shape[0]
    hidden = wg.shape[1]
    blk = NSP * CAP
    tile = model // NT

    def sp_at(d):
        return ((z + d // NX) % NZ) * NX + (x + d % NX) % NX

    def sp_back(d):
        return ((z - d // NX + NZ) % NZ) * NX + (x - d % NX + NX) % NX

    def tp_at(o):
        return ((y + o // 2) % 4) * 2 + (c + o % 2) % 2

    def tp_from(o):
        return ((y - o // 2 + 4) % 4) * 2 + (c - o % 2 + 2) % 2

    def remote(src, dst, ss, rs, dev):
        return pltpu.make_async_remote_copy(
            src_ref=src, dst_ref=dst, send_sem=ss, recv_sem=rs, device_id=dev, device_id_type=MESH
        )

    barrier = pltpu.get_barrier_semaphore()
    for d in range(1, NSP):
        pl.semaphore_signal(barrier, inc=1, device_id=(sp_at(d), tp), device_id_type=MESH)
    for o in range(1, NTP):
        pl.semaphore_signal(barrier, inc=1, device_id=(sp, tp_at(o)), device_id_type=MESH)

    local = [
        pltpu.make_async_copy(src, dst, lsem.at[i])
        for i, (src, dst) in enumerate(
            [
                (ig_h, ig), (va_h, va), (cw_h, cw), (doc_h, doc), (og_h, og), (rt_h, rt), (rw_h, rw),
                (stream_h, stream), (ng_h, ng), (nb_h, nb), (ow_h, ow),
                (wg_h.at[0], wg), (wu_h.at[0], wu), (wd_h.at[0], wd),
            ]
        )
    ]
    for copy in local:
        copy.start()

    for i in range(4):
        local[i].wait()
    ext[8:8 + length, :width] = ig[...].astype(F32) * va[...].astype(F32)
    ext[8:8 + length, width:] = jnp.transpose(jnp.broadcast_to(doc[...].astype(F32), (128, length)))
    local[4].wait()
    pl.semaphore_wait(barrier, NSP - 1 + NTP - 1)
    nxt = (sp + 1) % NSP
    halo_copy = remote(ext.at[pl.ds(length, 8), :], halo, h_s, h_r, (nxt, tp))
    halo_copy.start()

    def mixed(r0, n):
        d0 = ext[8 + r0:8 + r0 + n, width:]
        keep1 = jnp.where(ext[7 + r0:7 + r0 + n, width:] == d0, 1.0, 0.0)
        keep2 = jnp.where(ext[6 + r0:6 + r0 + n, width:] == d0, 1.0, 0.0)
        keep1 = jnp.concatenate([keep1] * (width // 128), axis=1)
        keep2 = jnp.concatenate([keep2] * (width // 128), axis=1)
        conv = (
            cw[0:1, :] * ext[6 + r0:6 + r0 + n, :width] * keep2
            + cw[1:2, :] * ext[7 + r0:7 + r0 + n, :width] * keep1
            + cw[2:3, :] * ext[8 + r0:8 + r0 + n, :width]
        )
        return (og[r0:r0 + n, :].astype(F32) * conv).astype(BF16)

    for t in range(1, NTP):
        mx[t] = mixed(t * rows, rows)
    a_copies = [
        remote(mx.at[tp_at(o)], tr.at[o], a_s.at[o], a_r.at[o], (sp, tp_at(o))) for o in range(1, NTP)
    ]
    order = (4, 5, 2, 3, 6, 7, 1)
    for o in order:
        @pl.when(tp_at(o) != 0)
        def _():
            a_copies[o - 1].start()

    halo_copy.wait_recv()
    ext[0:8, :width] = halo[:, :width]
    ext[0:8, width:] = jnp.where(sp == 0, -1.0, halo[:, width:])
    mx[0] = mixed(0, rows)
    for o in order:
        @pl.when(tp_at(o) == 0)
        def _():
            a_copies[o - 1].start()

    local[5].wait()
    local[6].wait()

    def relative(k):
        e = rt[k:k + 1, :]
        return (((e >> 2) + (NZ - z)) & 3) * NX + (((e & 3) + (NX - x)) & 3)

    rel = [relative(0), relative(1)]
    lanes = lax.broadcasted_iota(jnp.int32, (NSP, rows), 0)
    hot = [jnp.where(lanes == r, 1.0, 0.0) for r in rel]
    upper = one_hot(
        lax.broadcasted_iota(jnp.int32, (rows, rows), 0) < lax.broadcasted_iota(jnp.int32, (rows, rows), 1)
    )
    prefix = jnp.dot((hot[0] + hot[1]).astype(BF16), upper, preferred_element_type=F32)
    slots = lax.broadcasted_iota(jnp.int32, (NSP * PAD, rows), 0)
    place = []
    for k in range(2):
        rank = jnp.sum(prefix * hot[k], axis=0, keepdims=True)
        slot = rel[k] * PAD + rank.astype(jnp.int32)
        place.append(jnp.where(slots == slot, 1.0, 0.0))

    for i in range(7, 11):
        local[i].wait()
    tr[0] = mx[tp]
    acc[...] = RESIDUAL * stream[...].astype(F32)

    def project(o, _):
        @pl.when(o > 0)
        def _():
            remote(mx.at[tp_at(o)], tr.at[o], a_s.at[o], a_r.at[o], (sp, tp_at(o))).wait_recv()

        start = pl.multiple_of(tp_from(o) * width, width)
        acc[...] += jnp.dot(tr[o], ow[pl.ds(start, width), :], preferred_element_type=F32)
        return 0

    lax.fori_loop(0, NTP, project, 0)
    normed[...] = layer_norm(acc[...], ng[0:1, :], nb[0:1, :]).astype(BF16)

    both = (place[0] + place[1]).astype(BF16)
    for n in range(NT):
        cols = slice(n * tile, (n + 1) * tile)
        packed = jnp.dot(both, normed[:, cols], preferred_element_type=F32)
        snd[:, :, cols] = packed.reshape(NSP, PAD, tile).astype(BF16)
    b_copies = {
        d: remote(snd.at[d], rcv.at[d], b_s.at[d], b_r.at[d], (sp_at(d), tp)) for d in range(1, NSP)
    }
    sp_order = (10, 9, 11, 6, 14, 5, 7, 13, 15, 2, 8, 1, 3, 4, 12)
    for d in sp_order:
        b_copies[d].start()
    rcv[0] = snd[0]
    for d in sp_order:
        b_copies[d].wait_recv()
    row_i = lax.broadcasted_iota(jnp.int32, (blk, NSP * PAD), 0)
    slot_i = lax.broadcasted_iota(jnp.int32, (blk, NSP * PAD), 1)
    squeeze = one_hot(slot_i == (row_i & (NSP - 1)) * PAD + (row_i >> 4))
    for n in range(NT):
        cols = slice(n * tile, (n + 1) * tile)
        padded = rcv[:, :, cols].astype(F32).reshape(NSP * PAD, tile).astype(BF16)
        xb[0:blk, cols] = jnp.dot(squeeze, padded, preferred_element_type=F32).astype(BF16)

    fdir = 1 - 2 * c
    up = (sp, ((y + fdir + 4) % 4) * 2 + c)
    down = (sp, ((y - fdir + 4) % 4) * 2 + c)
    mate = (sp, y * 2 + 1 - c)
    position = {0: 0, 4: 1, 1: 2, 2: 3, 5: 4, 6: 5, 3: 6, 7: 7}

    def block(j):
        return xb.at[pl.ds(position[j] * blk, blk), :]

    to_up = remote(block(0), block(1), g_s.at[0], g_r.at[0], up)
    to_down = remote(block(0), block(2), g_s.at[1], g_r.at[1], down)
    forward = remote(block(1), block(3), g_s.at[2], g_r.at[2], up)
    pair = [remote(block(j), block(4 + j), p_s.at[j], p_r.at[j], mate) for j in range(4)]
    to_up.start()
    to_down.start()
    pair[0].start()

    def gate_up(r0, m):
        def some(gw, uw):
            xs = xb[r0:r0 + m, :]
            gate = jnp.dot(xs, gw, preferred_element_type=F32)
            upp = jnp.dot(xs, uw, preferred_element_type=F32)
            return (gate / (1.0 + jnp.exp(-gate)) * upp).astype(BF16)

        full = hidden // 256

        def step(i, _):
            cols = pl.ds(pl.multiple_of(i * 256, 256), 256)
            hb[0:m, cols] = some(wg[:, cols], wu[:, cols])
            return 0

        lax.fori_loop(0, full, step, 0)
        if hidden % 256:
            cols = slice(full * 256, hidden)
            hb[0:m, cols] = some(wg[:, cols], wu[:, cols])

    def d2d(k, n):
        lo, size = ((0, 1), (1, 2), (3, 1))[k]
        view = (pl.ds(lo * blk, size * blk), pl.ds(n * tile, tile))
        return remote(pb.at[view], rd.at[view], d_s.at[k * NT + n], d_r.at[k * NT + n], mate)

    def down_tile(k, n):
        lo, size = ((0, 1), (1, 2), (3, 1))[k]
        cols = slice(n * tile, (n + 1) * tile)
        m = 2 * size * blk
        part = jnp.dot(hb[0:m, :], wd[:, cols], preferred_element_type=F32)
        pf[lo * blk:(lo + size) * blk, cols] = part[:size * blk]
        pb[lo * blk:(lo + size) * blk, cols] = part[size * blk:].astype(BF16)
        d2d(k, n).start()

    def cols_of(n):
        return (slice(None), pl.ds(n * tile, tile))

    def send3(n):
        return remote(q3.at[cols_of(n)], tq.at[cols_of(n)], s3_s.at[n], s3_r.at[n], down)

    def send2(n):
        return remote(q2.at[cols_of(n)], rb.at[cols_of(n)], s2_s.at[n], s2_r.at[n], up)

    def send1(n):
        return remote(q1.at[cols_of(n)], ra.at[cols_of(n)], s1_s.at[n], s1_r.at[n], down)

    def summed(j, n):
        cols = slice(n * tile, (n + 1) * tile)
        return pf[j * blk:(j + 1) * blk, cols] + rd[j * blk:(j + 1) * blk, cols].astype(F32)

    pair[0].wait_recv()
    local[11].wait()
    local[12].wait()
    gate_up(0, 2 * blk)
    local[13].wait()
    for n in range(NT):
        down_tile(0, n)

    to_up.wait_recv()
    forward.start()
    pair[1].start()
    to_down.wait_recv()
    pair[2].start()
    pair[1].wait_recv()
    pair[2].wait_recv()
    gate_up(2 * blk, 4 * blk)
    forward.wait_recv()
    pair[3].start()

    def finish2(n):
        d2d(1, n).wait_recv()
        q2[:, n * tile:(n + 1) * tile] = summed(2, n).astype(BF16)
        send2(n).start()

    for n in range(NT):
        down_tile(1, n)
        if n > 0:
            finish2(n - 1)
    finish2(NT - 1)

    pair[3].wait_recv()
    gate_up(6 * blk, 2 * blk)

    def finish3(n):
        d2d(2, n).wait_recv()
        q3[:, n * tile:(n + 1) * tile] = summed(3, n).astype(BF16)
        send3(n).start()

    for n in range(NT):
        down_tile(2, n)
        if n > 0:
            finish3(n - 1)
    finish3(NT - 1)
    for n in range(NT):
        send3(n).wait_recv()
        cols = slice(n * tile, (n + 1) * tile)
        q1[:, cols] = (summed(1, n) + tq[:, cols].astype(F32)).astype(BF16)
        send1(n).start()
    spread = one_hot(
        lax.broadcasted_iota(jnp.int32, (NSP * PAD, blk), 0)
        == (lax.broadcasted_iota(jnp.int32, (NSP * PAD, blk), 1) & (NSP - 1)) * PAD
        + (lax.broadcasted_iota(jnp.int32, (NSP * PAD, blk), 1) >> 4)
    )
    for n in range(NT):
        d2d(0, n).wait_recv()
        send2(n).wait_recv()
        send1(n).wait_recv()
        cols = slice(n * tile, (n + 1) * tile)
        total = (summed(0, n) + ra[:, cols].astype(F32) + rb[:, cols].astype(F32)).astype(BF16)
        wide = jnp.dot(spread, total, preferred_element_type=F32)
        snd2[:, :, cols] = wide.reshape(NSP, PAD, tile).astype(BF16)

    e_copies = {
        d: remote(snd2.at[d], ret.at[d], e_s.at[d], e_r.at[d], (sp_back(d), tp)) for d in range(1, NSP)
    }
    for d in sp_order:
        e_copies[d].start()
    ret[0] = snd2[0]
    eye = lax.broadcasted_iota(jnp.int32, (rows, rows), 0) == lax.broadcasted_iota(jnp.int32, (rows, rows), 1)
    weight = [
        jnp.sum(jnp.where(eye, rw[k:k + 1, :], 0.0), axis=1, keepdims=True) for k in range(2)
    ]
    place = [p.astype(BF16) for p in place]
    for d in sp_order:
        e_copies[d].wait_recv()
    for n in range(NT):
        cols = slice(n * tile, (n + 1) * tile)
        came = ret[:, :, cols].astype(F32).reshape(NSP * PAD, tile).astype(BF16)
        routed = [
            weight[k]
            * lax.dot_general(place[k], came, (((0,), (0,)), ((), ())), preferred_element_type=F32)
            for k in range(2)
        ]
        acc[:, cols] = RESIDUAL * normed[:, cols].astype(F32) + (routed[0] + routed[1])
    out_ref[...] = layer_norm(acc[...], ng[1:2, :], nb[1:2, :]).astype(BF16)

    halo_copy.wait_send()
    for copy in a_copies:
        copy.wait_send()
    for d in sp_order:
        b_copies[d].wait_send()
        e_copies[d].wait_send()
    for copy in (to_up, to_down, forward, *pair):
        copy.wait_send()
    for n in range(NT):
        for k in range(3):
            d2d(k, n).wait_send()
        send3(n).wait_send()
        send2(n).wait_send()
        send1(n).wait_send()


def shards(stream, out_gate, in_gate, values, conv_weight, out_weight, doc_ids, routes, route_weight,
           norm_gain, norm_bias, expert_gate, expert_up, expert_down):
    length, width = out_gate.shape
    rows, model = stream.shape
    hidden = expert_gate.shape[2]
    blk = NSP * CAP
    any_spec = pl.BlockSpec(memory_space=pl.ANY)
    dma = pltpu.SemaphoreType.DMA
    scratch = [
        pltpu.VMEM((rows, model), BF16),
        pltpu.VMEM((length, width), BF16),
        pltpu.VMEM((length, width), BF16),
        pltpu.VMEM((length, width), BF16),
        pltpu.VMEM((3, width), F32),
        pltpu.VMEM((model, model), BF16),
        pltpu.VMEM((1, length), jnp.int32),
        pltpu.VMEM((2, rows), jnp.int32),
        pltpu.VMEM((2, rows), F32),
        pltpu.VMEM((2, model), F32),
        pltpu.VMEM((2, model), F32),
        pltpu.VMEM((model, hidden), BF16),
        pltpu.VMEM((model, hidden), BF16),
        pltpu.VMEM((hidden, model), BF16),
        pltpu.VMEM((8 + length, width + 128), F32),
        pltpu.VMEM((8, width + 128), F32),
        pltpu.VMEM((NTP, rows, width), BF16),
        pltpu.VMEM((NTP, rows, width), BF16),
        pltpu.VMEM((rows, model), F32),
        pltpu.VMEM((rows, model), BF16),
        pltpu.VMEM((NSP, PAD, model), BF16),
        pltpu.VMEM((NSP, PAD, model), BF16),
        pltpu.VMEM((8 * blk, model), BF16),
        pltpu.VMEM((4 * blk, hidden), BF16),
        pltpu.VMEM((4 * blk, model), F32),
        pltpu.VMEM((4 * blk, model), BF16),
        pltpu.VMEM((4 * blk, model), BF16),
        pltpu.VMEM((blk, model), BF16),
        pltpu.VMEM((blk, model), BF16),
        pltpu.VMEM((blk, model), BF16),
        pltpu.VMEM((blk, model), BF16),
        pltpu.VMEM((blk, model), BF16),
        pltpu.VMEM((blk, model), BF16),
        pltpu.VMEM((NSP, PAD, model), BF16),
        pltpu.VMEM((NSP, PAD, model), BF16),
        dma((14,)), dma, dma, dma((NTP,)), dma((NTP,)), dma((NSP,)), dma((NSP,)),
        dma((3,)), dma((3,)), dma((4,)), dma((4,)), dma((3 * NT,)), dma((3 * NT,)),
        dma((NT,)), dma((NT,)), dma((NT,)), dma((NT,)), dma((NT,)), dma((NT,)),
        dma((NSP,)), dma((NSP,)),
    ]
    return pl.pallas_call(
        body,
        out_shape=jax.ShapeDtypeStruct((rows, model), BF16),
        in_specs=[any_spec] * 14,
        out_specs=pl.BlockSpec(memory_space=pltpu.VMEM),
        scratch_shapes=scratch,
        compiler_params=pltpu.CompilerParams(
            collective_id=0, has_side_effects=True, vmem_limit_bytes=60 * 1024 * 1024
        ),
        name="layer",
    )(
        stream, out_gate, in_gate, values, conv_weight, out_weight, doc_ids.reshape(1, -1),
        routes.T, route_weight.T, norm_gain, norm_bias, expert_gate, expert_up, expert_down,
    )


def solution(mesh):
    in_specs = (
        P(("sp", "tp"), None),
        P("sp", "tp"),
        P("sp", "tp"),
        P("sp", "tp"),
        P(None, "tp"),
        P(),
        P("sp"),
        P(("sp", "tp"), None),
        P(("sp", "tp"), None),
        P(),
        P(),
        P("sp", None, "tp"),
        P("sp", None, "tp"),
        P("sp", "tp", None),
    )
    out_specs = P(("sp", "tp"), None)
    return jax.shard_map(shards, mesh=mesh, in_specs=in_specs, out_specs=out_specs, check_vma=False)
```

```python
import jax
import jax.numpy as jnp
from jax import lax
from jax.experimental import pallas as pl
from jax.experimental.pallas import tpu as pltpu
from jax.sharding import PartitionSpec as P

MESH = pl.DeviceIdType.MESH
RESIDUAL = 1.6817928
NX = 4
NZ = 4
NSP = 16
NTP = 8
CAP = 5
LB = 8
NT = 4
LAG = 2
F32 = jnp.float32
BF16 = jnp.bfloat16


def layer_norm(v, gain, bias):
    mean = jnp.mean(v, axis=-1, keepdims=True)
    cent = v - mean
    var = jnp.mean(cent * cent, axis=-1, keepdims=True)
    return cent * lax.rsqrt(var + 1e-05) * gain + bias


def one_hot(cond):
    return jnp.where(cond, 1.0, 0.0).astype(BF16)


def body(
    stream_h, og_h, ig_h, va_h, cw_h, ow_h, doc_h, rt_h, rw_h, ng_h, nb_h, wg_h, wu_h, wd_h,
    out_ref,
    stream, og, ig, va, cw, ow, doc, rt, rw, ng, nb, wg, wu, wd,
    ext, edge, edges, first, firsts, mx, tr, acc, normed, snd, rcv, xb, hb, pf, pb, rd, q1, q2, ra, rb, snd2, ret,
    rt_o, rw_o, normed_o, snd_o, rcv_o, snd2_o, ret_o, part_o, part, turn,
    lsem, h_s, h_r, i_s, i_r, a_s, a_r, b_s, b_r, g_s, g_r, p_s, p_r, d_s, d_r, s2_s, s2_r, s1_s, s1_r, e_s, e_r,
    o_s, o_r, c_s, c_r, f_s, f_r,
):
    sp = lax.axis_index("sp")
    tp = lax.axis_index("tp")
    z, x = sp // NX, sp % NX
    y, c = tp // 2, tp % 2
    width = og.shape[1]
    length = og.shape[0]
    model = stream.shape[1]
    rows = stream.shape[0]
    hidden = wg.shape[1]
    blk = NSP * CAP
    tile = model // NT
    half = model // 2

    def sp_at(d):
        return ((z + d // NX) % NZ) * NX + (x + d % NX) % NX

    def sp_back(d):
        return ((z - d // NX + NZ) % NZ) * NX + (x - d % NX + NX) % NX

    def tp_at(o):
        return ((y + o // 2) % 4) * 2 + (c + o % 2) % 2

    def tp_from(o):
        return ((y - o // 2 + 4) % 4) * 2 + (c - o % 2 + 2) % 2

    def remote(src, dst, ss, rs, dev):
        return pltpu.make_async_remote_copy(
            src_ref=src, dst_ref=dst, send_sem=ss, recv_sem=rs, device_id=dev, device_id_type=MESH
        )

    barrier = pltpu.get_barrier_semaphore()
    for d in range(1, NSP):
        pl.semaphore_signal(barrier, inc=1, device_id=(sp_at(d), tp), device_id_type=MESH)
    for o in range(1, NTP):
        pl.semaphore_signal(barrier, inc=1, device_id=(sp, tp_at(o)), device_id_type=MESH)

    nxt = (sp + 1) % NSP
    prv = (sp + NSP - 1) % NSP

    @pl.when(tp != 0)
    def _():
        pl.semaphore_signal(barrier, inc=1, device_id=(nxt, 0), device_id_type=MESH)

    @pl.when(tp == 0)
    def _():
        for t in range(1, NTP):
            pl.semaphore_signal(barrier, inc=1, device_id=(prv, t), device_id_type=MESH)

    local = [
        pltpu.make_async_copy(src, dst, lsem.at[i])
        for i, (src, dst) in enumerate(
            [
                (ig_h, ig), (va_h, va), (cw_h, cw), (doc_h, doc), (og_h, og), (rt_h, rt), (rw_h, rw),
                (stream_h, stream), (ng_h, ng), (nb_h, nb), (ow_h, ow),
                (wg_h.at[0], wg), (wu_h.at[0], wu), (wd_h.at[0], wd),
            ]
        )
    ]
    for copy in local[:10]:
        copy.start()

    for i in range(4):
        local[i].wait()
    ext[0:8, :width] = jnp.zeros((8, width), F32)
    ext[0:8, width:] = jnp.full((8, 128), -1.0, F32)
    ext[8:8 + length, :width] = ig[...].astype(F32) * va[...].astype(F32)
    ext[8:8 + length, width:] = jnp.transpose(jnp.broadcast_to(doc[...].astype(F32), (128, length)))
    local[4].wait()
    local[10].start()
    tail = ext[length:length + 8, :width]
    edge[:, :width] = cw[0:1, :] * tail
    edge[:, width:2 * width] = cw[1:2, :] * tail
    edge[:, 2 * width:] = ext[length:length + 8, width:]

    @pl.when(tp != 0)
    def _():
        pl.semaphore_wait(barrier, NSP + NTP - 1)

    @pl.when(tp == 0)
    def _():
        pl.semaphore_wait(barrier, NSP + 2 * NTP - 3)

    halo_copy = remote(edge, edges.at[tp], h_s, h_r.at[tp], (nxt, 0))
    halo_copy.start()
    far = (sp, ((y + 2) % 4) * 2 + c)
    local[5].wait()
    local[6].wait()
    far_copies = [
        remote(src, dst, o_s.at[i], o_r.at[i], far)
        for i, (src, dst) in enumerate([(rt, rt_o), (rw, rw_o), (normed, normed_o), (part_o, part)])
    ]
    far_copies[0].start()
    far_copies[1].start()

    def convolved(r0, n):
        d0 = ext[8 + r0:8 + r0 + n, width:]
        keep1 = jnp.where(ext[7 + r0:7 + r0 + n, width:] == d0, 1.0, 0.0)
        keep2 = jnp.where(ext[6 + r0:6 + r0 + n, width:] == d0, 1.0, 0.0)
        keep1 = jnp.concatenate([keep1] * (width // 128), axis=1)
        keep2 = jnp.concatenate([keep2] * (width // 128), axis=1)
        return (
            cw[0:1, :] * ext[6 + r0:6 + r0 + n, :width] * keep2
            + cw[1:2, :] * ext[7 + r0:7 + r0 + n, :width] * keep1
            + cw[2:3, :] * ext[8 + r0:8 + r0 + n, :width]
        )

    first[:, :width] = og[0:8, :].astype(F32)
    first[:, width:] = convolved(0, 8)

    @pl.when(tp != 0)
    def _():
        remote(first, firsts.at[tp], i_s, i_r.at[tp], (sp, 0)).start()

    for t in range(NTP):
        mx[t] = (og[t * rows:(t + 1) * rows, :].astype(F32) * convolved(t * rows, rows)).astype(BF16)
    a_copies = [
        remote(mx.at[tp_at(o)], tr.at[o], a_s.at[o], a_r.at[o], (sp, tp_at(o))) for o in range(1, NTP)
    ]
    for o in (4, 5, 2, 3, 6, 7, 1):
        a_copies[o - 1].start()
    for copy in local[11:]:
        copy.start()

    lanes = lax.broadcasted_iota(jnp.int32, (NSP, rows), 0)
    upper = one_hot(
        lax.broadcasted_iota(jnp.int32, (rows, rows), 0) < lax.broadcasted_iota(jnp.int32, (rows, rows), 1)
    )
    slots = lax.broadcasted_iota(jnp.int32, (blk, rows), 0)
    eye = lax.broadcasted_iota(jnp.int32, (rows, rows), 0) == lax.broadcasted_iota(jnp.int32, (rows, rows), 1)

    def placed(table):
        rel = []
        for k in range(2):
            e = table[k:k + 1, :]
            rel.append((((e >> 2) + (NZ - z)) & 3) * NX + (((e & 3) + (NX - x)) & 3))
        hot = [jnp.where(lanes == r, 1.0, 0.0) for r in rel]
        prefix = jnp.dot((hot[0] + hot[1]).astype(BF16), upper, preferred_element_type=F32)
        place = []
        for k in range(2):
            rank = jnp.sum(prefix * hot[k], axis=0, keepdims=True)
            slot = rel[k] * CAP + rank.astype(jnp.int32)
            place.append(jnp.where(slots == slot, 1.0, 0.0))
        return place

    def weights(table):
        return [jnp.sum(jnp.where(eye, table[k:k + 1, :], 0.0), axis=1, keepdims=True) for k in range(2)]

    place = placed(rt)

    for i in range(7, 11):
        local[i].wait()
    tr[0] = mx[tp]
    acc[...] = RESIDUAL * stream[...].astype(F32)

    def arrive(o):
        remote(mx.at[tp_at(o)], tr.at[o], a_s.at[o], a_r.at[o], (sp, tp_at(o))).wait_recv()

    @pl.when(tp == 0)
    def _():
        firsts[0] = first[...]
        row = lax.broadcasted_iota(jnp.int32, (8, 128), 0)
        d0 = ext[8:16, width:]
        for o in range(NTP):
            if o > 0:
                arrive(o)
        for o in range(NTP):
            t = tp_from(o)
            if o > 0:
                remote(first, firsts.at[t], i_s, i_r.at[t], (sp, 0)).wait_recv()
            remote(edge, edges.at[t], h_s, h_r.at[t], (nxt, 0)).wait_recv()
            came = pltpu.roll(edges[t], 2, 0)
            near = pltpu.roll(edges[t], 1, 0)
            live = jnp.where(sp > 0, 1.0, 0.0)
            keep2 = jnp.where((came[:, 2 * width:] == d0) & (row < 2), live, 0.0)
            keep1 = jnp.where((near[:, 2 * width:] == d0) & (row < 1), live, 0.0)
            keep2 = jnp.concatenate([keep2] * (width // 128), axis=1)
            keep1 = jnp.concatenate([keep1] * (width // 128), axis=1)
            conv = firsts[t, :, width:] + came[:, :width] * keep2 + near[:, width:2 * width] * keep1
            tr[o, 0:8, :] = (firsts[t, :, :width] * conv).astype(BF16)

    def project(o, _):
        @pl.when((o > 0) & (tp != 0))
        def _():
            arrive(o)

        start = pl.multiple_of(tp_from(o) * width, width)
        acc[...] += jnp.dot(tr[o], ow[pl.ds(start, width), :], preferred_element_type=F32)
        return 0

    lax.fori_loop(0, NTP, project, 0)
    normed[...] = layer_norm(acc[...], ng[0:1, :], nb[0:1, :]).astype(BF16)

    far_copies[2].start()

    def fold(rows_f32, dst, h):
        for b in range(LB):
            turn[pl.ds(b, blk, stride=LB), :] = rows_f32[:, b * 128:(b + 1) * 128]
        dst[h] = turn[...].reshape(NSP, CAP * LB, 128).astype(BF16)

    def unfold(src, h):
        turn[...] = src[h].astype(F32).reshape(blk * LB, 128)
        return jnp.concatenate(
            [turn[pl.ds(b, blk, stride=LB), :].astype(BF16) for b in range(LB)], axis=1
        )

    def pack(place, src, dst, h):
        both = (place[0] + place[1]).astype(BF16)
        fold(jnp.dot(both, src[:, h * half:(h + 1) * half], preferred_element_type=F32), dst, h)

    def halves(src, dst, ss, rs, to):
        return [
            {
                d: remote(
                    src.at[h, d], dst.at[h, d],
                    ss.at[h * NSP + d], rs.at[h * NSP + d], (to(d), tp),
                )
                for d in range(1, NSP)
            }
            for h in range(2)
        ]

    sp_order = (10, 9, 11, 6, 14, 5, 7, 13, 15, 2, 8, 1, 3, 4, 12)
    b_copies = halves(snd, rcv, b_s, b_r, sp_at)
    c_copies = halves(snd_o, rcv_o, c_s, c_r, sp_at)
    e_copies = halves(snd2, ret, e_s, e_r, sp_back)
    f_copies = halves(snd2_o, ret_o, f_s, f_r, sp_back)

    def start_all(copies):
        for d in sp_order:
            copies[d].start()

    def arrive_all(copies):
        for d in sp_order:
            copies[d].wait_recv()

    for h in range(2):
        pack(place, normed, snd, h)
        start_all(b_copies[h])
        rcv[h, 0] = snd[h, 0]
    far_copies[0].wait_recv()
    far_copies[1].wait_recv()
    place_o = placed(rt_o)
    fdir = 1 - 2 * c
    up = (sp, ((y + fdir + 4) % 4) * 2 + c)
    down = (sp, ((y - fdir + 4) % 4) * 2 + c)
    mate = (sp, y * 2 + 1 - c)
    position = {0: 0, 4: 1, 1: 2, 2: 3, 5: 4, 6: 5, 3: 6, 7: 7}

    def settle(src, j, h):
        r0 = position[j] * blk
        xb[h, r0:r0 + blk, :] = unfold(src, h)

    def block(j, h):
        return xb.at[h, pl.ds(position[j] * blk, blk), :]

    to_up = [remote(block(0, h), block(1, h), g_s.at[h], g_r.at[h], up) for h in range(2)]
    to_down = [remote(block(0, h), block(2, h), g_s.at[2 + h], g_r.at[2 + h], down) for h in range(2)]
    pair = [
        [remote(block(j, h), block(4 + j, h), p_s.at[2 * j + h], p_r.at[2 * j + h], mate) for h in range(2)]
        for j in range(4)
    ]

    def gather_half(h):
        arrive_all(b_copies[h])
        settle(rcv, 0, h)
        pair[0][h].start()
        to_up[h].start()
        to_down[h].start()

    gather_half(0)
    far_copies[2].wait_recv()
    for h in range(2):
        pack(place_o, normed_o, snd_o, h)
        start_all(c_copies[h])
        rcv_o[h, 0] = snd_o[h, 0]
    gather_half(1)

    def gate_up(r0, m):
        def some(gw, uw):
            lo, hi = xb[0, r0:r0 + m, :], xb[1, r0:r0 + m, :]
            gate, upp = [
                jnp.dot(lo, w[:half], preferred_element_type=F32)
                + jnp.dot(hi, w[half:], preferred_element_type=F32)
                for w in (gw, uw)
            ]
            return (gate / (1.0 + jnp.exp(-gate)) * upp).astype(BF16)

        full = hidden // 256

        def step(i, _):
            cols = pl.ds(pl.multiple_of(i * 256, 256), 256)
            hb[0:m, cols] = some(wg[:, cols], wu[:, cols])
            return 0

        lax.fori_loop(0, full, step, 0, unroll=True)
        if hidden % 256:
            cols = slice(full * 256, hidden)
            hb[0:m, cols] = some(wg[:, cols], wu[:, cols])

    def d2d(k, n):
        lo, size = ((0, 1), (1, 2), (3, 1))[k]
        view = (n, pl.ds(lo * blk, size * blk))
        return remote(pb.at[view], rd.at[view], d_s.at[k * NT + n], d_r.at[k * NT + n], mate)

    def down_tile(k, n):
        lo, size = ((0, 1), (1, 2), (3, 1))[k]
        cols = slice(n * tile, (n + 1) * tile)
        m = 2 * size * blk
        part = jnp.dot(hb[0:m, :], wd[:, cols], preferred_element_type=F32)
        pf[n, lo * blk:(lo + size) * blk, :] = part[:size * blk]
        pb[n, lo * blk:(lo + size) * blk, :] = part[size * blk:].astype(BF16)
        d2d(k, n).start()

    def send2(n):
        return remote(q2.at[n], rb.at[n], s2_s.at[n], s2_r.at[n], up)

    def send1(n):
        return remote(q1.at[n], ra.at[n], s1_s.at[n], s1_r.at[n], down)

    def summed(j, n):
        return pf[n, j * blk:(j + 1) * blk, :] + rd[n, j * blk:(j + 1) * blk, :].astype(F32)

    pair[0][0].wait_recv()
    pair[0][1].wait_recv()
    local[11].wait()
    local[12].wait()
    gate_up(0, 2 * blk)
    local[13].wait()
    for n in range(NT):
        down_tile(0, n)

    for h in range(2):
        arrive_all(c_copies[h])
        settle(rcv_o, 3, h)
        pair[3][h].start()

    def pass_on(h):
        to_up[h].wait_recv()
        pair[1][h].start()
        to_down[h].wait_recv()
        pair[2][h].start()

    pass_on(0)
    pair[3][0].wait_recv()
    pair[3][1].wait_recv()
    gate_up(6 * blk, 2 * blk)
    pass_on(1)

    for n in range(NT):
        down_tile(2, n)
    for h in range(2):
        pair[1][h].wait_recv()
        pair[2][h].wait_recv()
    gate_up(2 * blk, 4 * blk)

    def finish2(n):
        d2d(1, n).wait_recv()
        q1[n] = summed(1, n).astype(BF16)
        send1(n).start()
        q2[n] = summed(2, n).astype(BF16)
        send2(n).start()

    for n in range(NT):
        down_tile(1, n)
        if n >= LAG:
            finish2(n - LAG)
    for n in range(NT - LAG, NT):
        finish2(n)
    per = NT // 2
    for h in range(2):
        sums = []
        for n in range(h * per, (h + 1) * per):
            d2d(2, n).wait_recv()
            sums.append(summed(3, n))
        fold(jnp.concatenate(sums, axis=1), snd2_o, h)
        start_all(f_copies[h])
        ret_o[h, 0] = snd2_o[h, 0]

    for h in range(2):
        sums = []
        for n in range(h * per, (h + 1) * per):
            d2d(0, n).wait_recv()
            send2(n).wait_recv()
            send1(n).wait_recv()
            sums.append(summed(0, n) + ra[n].astype(F32) + rb[n].astype(F32))
        fold(jnp.concatenate(sums, axis=1), snd2, h)
        start_all(e_copies[h])
        ret[h, 0] = snd2[h, 0]

    def picked(place, weight, src, h):
        came = unfold(src, h)
        routed = [
            weight[k] * lax.dot_general(
                place[k].astype(BF16), came, (((0,), (0,)), ((), ())), preferred_element_type=F32
            )
            for k in range(2)
        ]
        return routed[0] + routed[1]

    weight_o = weights(rw_o)
    weight = weights(rw)
    for h in range(2):
        arrive_all(f_copies[h])
        part_o[:, h * half:(h + 1) * half] = picked(place_o, weight_o, ret_o, h).astype(BF16)
    far_copies[3].start()
    for h in range(2):
        cols = slice(h * half, (h + 1) * half)
        arrive_all(e_copies[h])
        acc[:, cols] = RESIDUAL * normed[:, cols].astype(F32) + picked(place, weight, ret, h)
    far_copies[3].wait_recv()
    acc[...] += part[...].astype(F32)
    out_ref[...] = layer_norm(acc[...], ng[1:2, :], nb[1:2, :]).astype(BF16)

    halo_copy.wait_send()

    @pl.when(tp != 0)
    def _():
        remote(first, firsts.at[tp], i_s, i_r.at[tp], (sp, 0)).wait_send()

    for copy in (*a_copies, *far_copies, *to_up, *to_down, *pair[0], *pair[1], *pair[2], *pair[3]):
        copy.wait_send()
    for d in sp_order:
        for h in range(2):
            for copies in (b_copies, c_copies, e_copies, f_copies):
                copies[h][d].wait_send()
    for n in range(NT):
        for k in range(3):
            d2d(k, n).wait_send()
        send2(n).wait_send()
        send1(n).wait_send()


def shards(stream, out_gate, in_gate, values, conv_weight, out_weight, doc_ids, routes, route_weight,
           norm_gain, norm_bias, expert_gate, expert_up, expert_down):
    length, width = out_gate.shape
    rows, model = stream.shape
    hidden = expert_gate.shape[2]
    blk = NSP * CAP
    any_spec = pl.BlockSpec(memory_space=pltpu.HBM)
    dma = pltpu.SemaphoreType.DMA
    scratch = [
        pltpu.VMEM((rows, model), BF16),
        pltpu.VMEM((length, width), BF16),
        pltpu.VMEM((length, width), BF16),
        pltpu.VMEM((length, width), BF16),
        pltpu.VMEM((3, width), F32),
        pltpu.VMEM((model, model), BF16),
        pltpu.VMEM((1, length), jnp.int32),
        pltpu.VMEM((2, rows), jnp.int32),
        pltpu.VMEM((2, rows), F32),
        pltpu.VMEM((2, model), F32),
        pltpu.VMEM((2, model), F32),
        pltpu.VMEM((model, hidden), BF16),
        pltpu.VMEM((model, hidden), BF16),
        pltpu.VMEM((hidden, model), BF16),
        pltpu.VMEM((8 + length, width + 128), F32),
        pltpu.VMEM((8, 2 * width + 128), F32),
        pltpu.VMEM((NTP, 8, 2 * width + 128), F32),
        pltpu.VMEM((8, 2 * width), F32),
        pltpu.VMEM((NTP, 8, 2 * width), F32),
        pltpu.VMEM((NTP, rows, width), BF16),
        pltpu.VMEM((NTP, rows, width), BF16),
        pltpu.VMEM((rows, model), F32),
        pltpu.VMEM((rows, model), BF16),
        pltpu.VMEM((2, NSP, CAP * LB, 128), BF16),
        pltpu.VMEM((2, NSP, CAP * LB, 128), BF16),
        pltpu.VMEM((2, 8 * blk, model // 2), BF16),
        pltpu.VMEM((4 * blk, hidden), BF16),
        pltpu.VMEM((NT, 4 * blk, model // NT), F32),
        pltpu.VMEM((NT, 4 * blk, model // NT), BF16),
        pltpu.VMEM((NT, 4 * blk, model // NT), BF16),
        pltpu.VMEM((NT, blk, model // NT), BF16),
        pltpu.VMEM((NT, blk, model // NT), BF16),
        pltpu.VMEM((NT, blk, model // NT), BF16),
        pltpu.VMEM((NT, blk, model // NT), BF16),
        pltpu.VMEM((2, NSP, CAP * LB, 128), BF16),
        pltpu.VMEM((2, NSP, CAP * LB, 128), BF16),
        pltpu.VMEM((2, rows), jnp.int32),
        pltpu.VMEM((2, rows), F32),
        pltpu.VMEM((rows, model), BF16),
        pltpu.VMEM((2, NSP, CAP * LB, 128), BF16),
        pltpu.VMEM((2, NSP, CAP * LB, 128), BF16),
        pltpu.VMEM((2, NSP, CAP * LB, 128), BF16),
        pltpu.VMEM((2, NSP, CAP * LB, 128), BF16),
        pltpu.VMEM((rows, model), BF16),
        pltpu.VMEM((rows, model), BF16),
        pltpu.VMEM((blk * LB, 128), F32),
        dma((14,)), dma, dma((NTP,)), dma, dma((NTP,)), dma((NTP,)), dma((NTP,)), dma((2 * NSP,)), dma((2 * NSP,)),
        dma((4,)), dma((4,)), dma((8,)), dma((8,)), dma((3 * NT,)), dma((3 * NT,)),
        dma((NT,)), dma((NT,)), dma((NT,)), dma((NT,)),
        dma((2 * NSP,)), dma((2 * NSP,)),
        dma((4,)), dma((4,)), dma((2 * NSP,)), dma((2 * NSP,)), dma((2 * NSP,)), dma((2 * NSP,)),
    ]
    return pl.pallas_call(
        body,
        out_shape=jax.ShapeDtypeStruct((rows, model), BF16),
        in_specs=[any_spec] * 14,
        out_specs=pl.BlockSpec(memory_space=pltpu.VMEM),
        scratch_shapes=scratch,
        compiler_params=pltpu.CompilerParams(
            collective_id=0, has_side_effects=True, vmem_limit_bytes=48 * 1024 * 1024
        ),
        name="layer",
    )(*[pltpu.with_memory_space_constraint(v, pltpu.HBM) for v in (
        stream, out_gate, in_gate, values, conv_weight, out_weight, doc_ids.reshape(1, -1),
        routes.T, route_weight.T, norm_gain, norm_bias, expert_gate, expert_up, expert_down,
    )])


def solution(mesh):
    in_specs = (
        P(("sp", "tp"), None),
        P("sp", "tp"),
        P("sp", "tp"),
        P("sp", "tp"),
        P(None, "tp"),
        P(),
        P("sp"),
        P(("sp", "tp"), None),
        P(("sp", "tp"), None),
        P(),
        P(),
        P("sp", None, "tp"),
        P("sp", None, "tp"),
        P("sp", "tp", None),
    )
    out_specs = P(("sp", "tp"), None)
    return jax.shard_map(shards, mesh=mesh, in_specs=in_specs, out_specs=out_specs, check_vma=False)
```

```python
import jax
import jax.numpy as jnp
from jax import lax
from jax.experimental import pallas as pl
from jax.experimental.pallas import tpu as pltpu
from jax.sharding import PartitionSpec as P

MESH = pl.DeviceIdType.MESH
RESIDUAL = 1.6817928
NX = 4
NZ = 4
NSP = 16
NTP = 8
CAP = 5
LB = 8
NT = 4
F32 = jnp.float32
BF16 = jnp.bfloat16


def layer_norm(v, gain, bias):
    mean = jnp.mean(v, axis=-1, keepdims=True)
    cent = v - mean
    var = jnp.mean(cent * cent, axis=-1, keepdims=True)
    return cent * lax.rsqrt(var + 1e-05) * gain + bias


def one_hot(cond):
    return jnp.where(cond, 1.0, 0.0).astype(BF16)


def body(
    stream_h, og_h, ig_h, va_h, cw_h, ow_h, doc_h, rt_h, rw_h, ng_h, nb_h, wg_h, wu_h, wd_h,
    out_ref,
    stream, og, ig, va, cw, ow, doc, rt, rw, ng, nb, wg, wu, wd,
    ext, halo, term, terms, mx, tr, acc, normed, snd, rcv, xb, hb, pf, pb, rd, q, rab, snd2, ret,
    rt_o, rw_o, normed_o, snd_o, rcv_o, snd2_o, ret_o, part_o, part, turn,
    lsem, h_s, h_r, i_s, i_r, a_s, a_r, b_s, b_r, g_s, g_r, p_s, p_r, d_s, d_r, q_s, q_r, e_s, e_r,
    o_s, o_r, c_s, c_r, f_s, f_r,
):
    sp = lax.axis_index("sp")
    tp = lax.axis_index("tp")
    z, x = sp // NX, sp % NX
    y, c = tp // 2, tp % 2
    width = og.shape[1]
    length = og.shape[0]
    model = stream.shape[1]
    rows = stream.shape[0]
    hidden = wg.shape[1]
    blk = NSP * CAP
    tile = model // NT
    half = model // 2
    per = NT // 2

    def sp_at(d):
        return ((z + d // NX) % NZ) * NX + (x + d % NX) % NX

    def sp_back(d):
        return ((z - d // NX + NZ) % NZ) * NX + (x - d % NX + NX) % NX

    def tp_at(o):
        return ((y + o // 2) % 4) * 2 + (c + o % 2) % 2

    def tp_from(o):
        return ((y - o // 2 + 4) % 4) * 2 + (c - o % 2 + 2) % 2

    def remote(src, dst, ss, rs, dev):
        return pltpu.make_async_remote_copy(
            src_ref=src, dst_ref=dst, send_sem=ss, recv_sem=rs, device_id=dev, device_id_type=MESH
        )

    def whole(ref, sem):
        remote(ref, ref, sem, sem, (sp, tp)).wait_recv()

    barrier = pltpu.get_barrier_semaphore()
    for d in range(1, NSP):
        pl.semaphore_signal(barrier, inc=1, device_id=(sp_at(d), tp), device_id_type=MESH)
    for o in range(1, NTP):
        pl.semaphore_signal(barrier, inc=1, device_id=(sp, tp_at(o)), device_id_type=MESH)

    nxt = (sp + 1) % NSP

    local = [
        pltpu.make_async_copy(src, dst, lsem.at[i])
        for i, (src, dst) in enumerate(
            [
                (ig_h, ig), (va_h, va), (cw_h, cw), (doc_h, doc), (og_h, og), (rt_h, rt), (rw_h, rw),
                (stream_h, stream), (ng_h, ng), (nb_h, nb), (ow_h, ow),
                (wg_h.at[0], wg), (wu_h.at[0], wu), (wd_h.at[0], wd),
            ]
        )
    ]
    for copy in local[:10]:
        copy.start()

    for i in range(4):
        local[i].wait()
    ext[0:8, :width] = jnp.zeros((8, width), F32)
    ext[0:8, width:] = jnp.full((8, 128), -1.0, F32)
    ext[8:8 + length, :width] = ig[...].astype(F32) * va[...].astype(F32)
    ext[8:8 + length, width:] = jnp.transpose(jnp.broadcast_to(doc[...].astype(F32), (128, length)))
    local[4].wait()
    local[10].start()
    pl.semaphore_wait(barrier, NSP + NTP - 2)
    halo_copy = remote(ext.at[pl.ds(length, 8), :], halo, h_s, h_r, (nxt, tp))
    halo_copy.start()
    far = (sp, ((y + 2) % 4) * 2 + c)
    local[5].wait()
    local[6].wait()
    far_copies = [
        remote(src, dst, o_s.at[i], o_r.at[i], far)
        for i, (src, dst) in enumerate([
            (rt, rt_o), (rw, rw_o),
            (normed.at[:, pl.ds(0, half)], normed_o.at[:, pl.ds(0, half)]),
            (normed.at[:, pl.ds(half, half)], normed_o.at[:, pl.ds(half, half)]),
            (part_o, part),
        ])
    ]
    far_copies[0].start()
    far_copies[1].start()

    def convolved(r0, n):
        d0 = ext[8 + r0:8 + r0 + n, width:]
        keep1 = jnp.where(ext[7 + r0:7 + r0 + n, width:] == d0, 1.0, 0.0)
        keep2 = jnp.where(ext[6 + r0:6 + r0 + n, width:] == d0, 1.0, 0.0)
        keep1 = jnp.concatenate([keep1] * (width // 128), axis=1)
        keep2 = jnp.concatenate([keep2] * (width // 128), axis=1)
        return (
            cw[0:1, :] * ext[6 + r0:6 + r0 + n, :width] * keep2
            + cw[1:2, :] * ext[7 + r0:7 + r0 + n, :width] * keep1
            + cw[2:3, :] * ext[8 + r0:8 + r0 + n, :width]
        )

    for t in range(NTP):
        mx[t] = (og[t * rows:(t + 1) * rows, :].astype(F32) * convolved(t * rows, rows)).astype(BF16)
    a_copies = [
        remote(mx.at[tp_at(o)], tr.at[o], a_s, a_r.at[o], (sp, tp_at(o))) for o in range(1, NTP)
    ]
    for o in (4, 5, 2, 3, 6, 7, 1):
        a_copies[o - 1].start()
    for copy in local[11:]:
        copy.start()

    lanes = lax.broadcasted_iota(jnp.int32, (NSP, rows), 0)
    upper = one_hot(
        lax.broadcasted_iota(jnp.int32, (rows, rows), 0) < lax.broadcasted_iota(jnp.int32, (rows, rows), 1)
    )
    slots = lax.broadcasted_iota(jnp.int32, (blk, rows), 0)
    eye = lax.broadcasted_iota(jnp.int32, (rows, rows), 0) == lax.broadcasted_iota(jnp.int32, (rows, rows), 1)

    def placed(table):
        rel = []
        for k in range(2):
            e = table[k:k + 1, :]
            rel.append((((e >> 2) + (NZ - z)) & 3) * NX + (((e & 3) + (NX - x)) & 3))
        hot = [jnp.where(lanes == r, 1.0, 0.0) for r in rel]
        prefix = jnp.dot((hot[0] + hot[1]).astype(BF16), upper, preferred_element_type=F32)
        place = []
        for k in range(2):
            rank = jnp.sum(prefix * hot[k], axis=0, keepdims=True)
            slot = rel[k] * CAP + rank.astype(jnp.int32)
            place.append(jnp.where(slots == slot, 1.0, 0.0))
        return place

    def weights(table):
        return [jnp.sum(jnp.where(eye, table[k:k + 1, :], 0.0), axis=1, keepdims=True) for k in range(2)]

    place = placed(rt)

    for i in range(7, 11):
        local[i].wait()

    def project(lhs, t):
        start = pl.multiple_of(t * width, width)
        return jnp.dot(lhs, ow[pl.ds(start, width), :], preferred_element_type=F32)

    acc[...] = RESIDUAL * stream[...].astype(F32) + project(mx[tp], tp)
    halo_copy.wait_recv()
    ext[0:8, :width] = halo[:, :width]
    ext[0:8, width:] = jnp.where(sp == 0, -1.0, halo[:, width:])
    fixed = (og[0:16, :].astype(F32) * convolved(0, 16)).astype(BF16)
    term[...] = project(fixed, tp)[0:2, :]

    @pl.when(tp != 0)
    def _():
        remote(term, terms.at[tp], i_s, i_r, (sp, 0)).start()

    for o in (1, 2, 3, 6, 7, 4, 5):
        a_copies[o - 1].wait_recv()
        acc[...] += project(tr[o], tp_from(o))

    @pl.when(tp == 0)
    def _():
        whole(terms.at[pl.ds(1, NTP - 1)], i_r)
        total = term[...]
        for t in range(1, NTP):
            total += terms[t]
        acc[0:2, :] = RESIDUAL * stream[0:2, :].astype(F32) + total

    normed[...] = layer_norm(acc[...], ng[0:1, :], nb[0:1, :]).astype(BF16)

    far_copies[2].start()
    far_copies[3].start()

    def fold(rows_f32, dst, h):
        for b in range(LB):
            turn[pl.ds(b, blk, stride=LB), :] = rows_f32[:, b * 128:(b + 1) * 128]
        dst[h] = turn[...].reshape(NSP, CAP * LB, 128).astype(BF16)

    def unfold(src, h):
        turn[...] = src[h].astype(F32).reshape(blk * LB, 128)
        return jnp.concatenate(
            [turn[pl.ds(b, blk, stride=LB), :].astype(BF16) for b in range(LB)], axis=1
        )

    def pack(place, src, dst, h):
        both = (place[0] + place[1]).astype(BF16)
        fold(jnp.dot(both, src[:, h * half:(h + 1) * half], preferred_element_type=F32), dst, h)

    def halves(src, dst, ss, rs, to):
        return [
            {
                d: remote(src.at[h, d], dst.at[h, d], ss, rs.at[h], (to(d), tp))
                for d in range(1, NSP)
            }
            for h in range(2)
        ]

    sp_order = (10, 9, 11, 6, 14, 5, 7, 13, 15, 2, 8, 1, 3, 4, 12)
    b_copies = halves(snd, rcv, b_s, b_r, sp_at)
    c_copies = halves(snd_o, rcv_o, c_s, c_r, sp_at)
    e_copies = halves(snd2, ret, e_s, e_r, sp_back)
    f_copies = halves(snd2_o, ret_o, f_s, f_r, sp_back)

    def start_all(copies):
        for d in sp_order:
            copies[d].start()

    def arrive_all(dst, rs, h):
        whole(dst.at[h, pl.ds(1, NSP - 1)], rs.at[h])

    for h in range(2):
        pack(place, normed, snd, h)
        start_all(b_copies[h])
        rcv[h, 0] = snd[h, 0]
    far_copies[0].wait_recv()
    far_copies[1].wait_recv()
    place_o = placed(rt_o)
    def side_of(row):
        return (1 - 2 * c) * (1 - 2 * (row // 3))

    side = side_of(y)
    above, below = (y + 1) % 4, (y + 3) % 4
    first_above = side_of(above) == -1
    first_below = side_of(below) == 1
    toward = [(sp, ((y + side + 4) % 4) * 2 + c), (sp, ((y - side + 4) % 4) * 2 + c)]
    mate = (sp, y * 2 + 1 - c)
    position = {0: 0, 4: 1, 3: 2, 7: 3, 1: 4, 5: 5, 2: 6, 6: 7}

    def settle(src, j, h):
        r0 = position[j] * blk
        xb[h, r0:r0 + blk, :] = unfold(src, h)

    def block(j, h):
        return xb.at[h, pl.ds(position[j] * blk, blk), :]

    def neighbour(row, is_first, h):
        k = jnp.where(is_first, 0, 1)
        rows_at = pl.multiple_of((position[1] + k * (position[2] - position[1])) * blk, blk)
        return remote(
            block(0, h), xb.at[h, pl.ds(rows_at, blk), :], g_s, g_r.at[2 * k + h], (sp, row * 2 + c)
        )

    to_near = [
        (first_above, [neighbour(above, first_above, h) for h in range(2)]),
        (first_below, [neighbour(below, first_below, h) for h in range(2)]),
    ]

    def from_near(j, h):
        remote(block(0, h), block(j, h), g_s, g_r.at[2 * (j - 1) + h], mate).wait_recv()

    pair = [
        [remote(block(j, h), block(4 + j, h), p_s, p_r.at[j], mate) for h in range(2)]
        for j in range(4)
    ]

    def gather_half(h):
        arrive_all(rcv, b_r, h)
        settle(rcv, 0, h)
        pair[0][h].start()
        for is_first, copies in to_near:
            @pl.when(is_first)
            def _():
                copies[h].start()

    def far_dispatch():
        for h in range(2):
            far_copies[2 + h].wait_recv()
            pack(place_o, normed_o, snd_o, h)
            start_all(c_copies[h])
            rcv_o[h, 0] = snd_o[h, 0]

    pl.when(tp == 0)(far_dispatch)
    gather_half(0)
    pl.when((tp != 0) & (tp != 4))(far_dispatch)
    gather_half(1)
    pl.when(tp == 4)(far_dispatch)

    def gate_up(j, between=()):
        r0 = position[j] * blk
        lo, hi = (xb.at[h, pl.ds(r0, 2 * blk), :] for h in range(2))
        for i, c0 in enumerate(range(0, hidden, 256)):
            cols = slice(c0, min(c0 + 256, hidden))
            gate, upp = [
                jnp.dot(lo[...], w[:half, cols], preferred_element_type=F32)
                + jnp.dot(hi[...], w[half:, cols], preferred_element_type=F32)
                for w in (wg, wu)
            ]
            hb[:, cols] = (gate / (1.0 + jnp.exp(-gate)) * upp).astype(BF16)
            if i < len(between) and between[i]:
                between[i]()

    def d2d(j, n):
        view = (n, pl.ds(j * blk, blk))
        return remote(pb.at[view], rd.at[view], d_s, d_r.at[2 * j + n // per], mate)

    def d2d_in(j, h):
        whole(rd.at[pl.ds(h * per, per), pl.ds(j * blk, blk)], d_r.at[2 * j + h])

    def pair_in(j):
        whole(xb.at[:, pl.ds(position[4 + j] * blk, blk)], p_r.at[j])

    def down_tiles(j, tiles):
        for n in tiles:
            part = jnp.dot(hb[...], wd[:, n * tile:(n + 1) * tile], preferred_element_type=F32)
            pf[n, j * blk:(j + 1) * blk, :] = part[:blk]
            pb[n, j * blk:(j + 1) * blk, :] = part[blk:].astype(BF16)
        for n in tiles:
            d2d(j, n).start()

    behind = (1 + side) // 2

    def send(j, n):
        k = behind if j == 1 else 1 - behind
        return remote(q.at[j - 1, n], rab.at[k, n], q_s, q_r.at[2 * k + n // per], toward[j - 1])

    def summed(j, n):
        return pf[n, j * blk:(j + 1) * blk, :] + rd[n, j * blk:(j + 1) * blk, :].astype(F32)

    def finish(j, h):
        d2d_in(j, h)
        for n in range(h * per, (h + 1) * per):
            q[j - 1, n] = summed(j, n).astype(BF16)
            send(j, n).start()

    def far_total(h):
        d2d_in(3, h)
        fold(jnp.concatenate([summed(3, n) for n in range(h * per, (h + 1) * per)], axis=1), snd2_o, h)
        start_all(f_copies[h])
        ret_o[h, 0] = snd2_o[h, 0]

    def down_pass(j):
        down_tiles(j, range(per))
        down_tiles(j, range(per, NT))

    local[11].wait()
    local[12].wait()
    local[13].wait()
    @pl.when(y != 0)
    def _():
        pair_in(0)
        gate_up(0)

    from_near(1, 0)
    pair[1][0].start()
    from_near(1, 1)
    pair[1][1].start()
    for is_first, copies in to_near:
        @pl.when(jnp.logical_not(is_first))
        def _():
            copies[0].start()
            copies[1].start()
    @pl.when(y != 0)
    def _():
        down_tiles(0, range(NT))

    for h in range(2):
        arrive_all(rcv_o, c_r, h)
        settle(rcv_o, 3, h)
        pair[3][h].start()
    pair_in(1)
    gate_up(1)
    down_pass(1)
    pair_in(3)
    gate_up(3, (None, lambda: finish(1, 0), lambda: finish(1, 1)))
    for h in range(2):
        from_near(2, h)
        pair[2][h].start()
    down_pass(3)
    pair_in(2)
    gate_up(2, (None, lambda: far_total(0), lambda: far_total(1)))
    down_pass(2)
    @pl.when(y == 0)
    def _():
        pair_in(0)
        gate_up(0, (None, lambda: finish(2, 0), lambda: finish(2, 1)))
        down_pass(0)

    @pl.when(y != 0)
    def _():
        finish(2, 0)
        finish(2, 1)

    def picked(place, weight, src, h):
        came = unfold(src, h)
        routed = [
            weight[k] * lax.dot_general(
                place[k].astype(BF16), came, (((0,), (0,)), ((), ())), preferred_element_type=F32
            )
            for k in range(2)
        ]
        return routed[0] + routed[1]

    weight_o = weights(rw_o)
    weight = weights(rw)

    def own_total(h):
        d2d_in(0, h)
        for k in range(2):
            whole(rab.at[k, pl.ds(h * per, per)], q_r.at[2 * k + h])
        sums = [
            summed(0, n) + rab[0, n].astype(F32) + rab[1, n].astype(F32)
            for n in range(h * per, (h + 1) * per)
        ]
        fold(jnp.concatenate(sums, axis=1), snd2, h)
        start_all(e_copies[h])
        ret[h, 0] = snd2[h, 0]

    own_total(0)
    for h in range(2):
        arrive_all(ret_o, f_r, h)
        part_o[:, h * half:(h + 1) * half] = picked(place_o, weight_o, ret_o, h).astype(BF16)
    far_copies[4].start()
    own_total(1)
    halo_copy.wait_send()

    @pl.when(tp != 0)
    def _():
        remote(term, terms.at[tp], i_s, i_r, (sp, 0)).wait_send()

    for copy in far_copies[:4]:
        copy.wait_send()
    whole(mx.at[pl.ds(1, NTP - 1)], a_s)
    for src, ss in ((snd, b_s), (snd_o, c_s), (snd2_o, f_s)):
        whole(src.at[:, pl.ds(1, NSP - 1)], ss)
    whole(xb.at[0, pl.ds(0, 4 * blk)], g_s)
    whole(xb.at[0], p_s)
    whole(pb, d_s)
    whole(q, q_s)
    for h in range(2):
        cols = slice(h * half, (h + 1) * half)
        arrive_all(ret, e_r, h)
        acc[:, cols] = RESIDUAL * normed[:, cols].astype(F32) + picked(place, weight, ret, h)
    far_copies[4].wait_recv()
    acc[...] += part[...].astype(F32)
    out_ref[...] = layer_norm(acc[...], ng[1:2, :], nb[1:2, :]).astype(BF16)

    far_copies[4].wait_send()
    whole(snd2.at[:, pl.ds(1, NSP - 1)], e_s)


def shards(stream, out_gate, in_gate, values, conv_weight, out_weight, doc_ids, routes, route_weight,
           norm_gain, norm_bias, expert_gate, expert_up, expert_down):
    length, width = out_gate.shape
    rows, model = stream.shape
    hidden = expert_gate.shape[2]
    blk = NSP * CAP
    any_spec = pl.BlockSpec(memory_space=pltpu.HBM)
    dma = pltpu.SemaphoreType.DMA
    scratch = [
        pltpu.VMEM((rows, model), BF16),
        pltpu.VMEM((length, width), BF16),
        pltpu.VMEM((length, width), BF16),
        pltpu.VMEM((length, width), BF16),
        pltpu.VMEM((3, width), F32),
        pltpu.VMEM((model, model), BF16),
        pltpu.VMEM((1, length), jnp.int32),
        pltpu.VMEM((2, rows), jnp.int32),
        pltpu.VMEM((2, rows), F32),
        pltpu.VMEM((2, model), F32),
        pltpu.VMEM((2, model), F32),
        pltpu.VMEM((model, hidden), BF16),
        pltpu.VMEM((model, hidden), BF16),
        pltpu.VMEM((hidden, model), BF16),
        pltpu.VMEM((8 + length, width + 128), F32),
        pltpu.VMEM((8, width + 128), F32),
        pltpu.VMEM((2, model), F32),
        pltpu.VMEM((NTP, 2, model), F32),
        pltpu.VMEM((NTP, rows, width), BF16),
        pltpu.VMEM((NTP, rows, width), BF16),
        pltpu.VMEM((rows, model), F32),
        pltpu.VMEM((rows, model), BF16),
        pltpu.VMEM((2, NSP, CAP * LB, 128), BF16),
        pltpu.VMEM((2, NSP, CAP * LB, 128), BF16),
        pltpu.VMEM((2, 8 * blk, model // 2), BF16),
        pltpu.VMEM((2 * blk, hidden), BF16),
        pltpu.VMEM((NT, 4 * blk, model // NT), F32),
        pltpu.VMEM((NT, 4 * blk, model // NT), BF16),
        pltpu.VMEM((NT, 4 * blk, model // NT), BF16),
        pltpu.VMEM((2, NT, blk, model // NT), BF16),
        pltpu.VMEM((2, NT, blk, model // NT), BF16),
        pltpu.VMEM((2, NSP, CAP * LB, 128), BF16),
        pltpu.VMEM((2, NSP, CAP * LB, 128), BF16),
        pltpu.VMEM((2, rows), jnp.int32),
        pltpu.VMEM((2, rows), F32),
        pltpu.VMEM((rows, model), BF16),
        pltpu.VMEM((2, NSP, CAP * LB, 128), BF16),
        pltpu.VMEM((2, NSP, CAP * LB, 128), BF16),
        pltpu.VMEM((2, NSP, CAP * LB, 128), BF16),
        pltpu.VMEM((2, NSP, CAP * LB, 128), BF16),
        pltpu.VMEM((rows, model), BF16),
        pltpu.VMEM((rows, model), BF16),
        pltpu.VMEM((blk * LB, 128), F32),
        dma((14,)), dma, dma, dma, dma, dma, dma((NTP,)), dma, dma((2,)),
        dma, dma((4,)), dma, dma((4,)), dma, dma((8,)),
        dma, dma((4,)), dma, dma((2,)),
        dma((5,)), dma((5,)), dma, dma((2,)), dma, dma((2,)),
    ]
    return pl.pallas_call(
        body,
        out_shape=jax.ShapeDtypeStruct((rows, model), BF16),
        in_specs=[any_spec] * 14,
        out_specs=pl.BlockSpec(memory_space=pltpu.VMEM),
        scratch_shapes=scratch,
        compiler_params=pltpu.CompilerParams(
            collective_id=0, has_side_effects=True, vmem_limit_bytes=48 * 1024 * 1024
        ),
        name="layer",
    )(*[pltpu.with_memory_space_constraint(v, pltpu.HBM) for v in (
        stream, out_gate, in_gate, values, conv_weight, out_weight, doc_ids.reshape(1, -1),
        routes.T, route_weight.T, norm_gain, norm_bias, expert_gate, expert_up, expert_down,
    )])


def solution(mesh):
    in_specs = (
        P(("sp", "tp"), None),
        P("sp", "tp"),
        P("sp", "tp"),
        P("sp", "tp"),
        P(None, "tp"),
        P(),
        P("sp"),
        P(("sp", "tp"), None),
        P(("sp", "tp"), None),
        P(),
        P(),
        P("sp", None, "tp"),
        P("sp", None, "tp"),
        P("sp", "tp", None),
    )
    out_specs = P(("sp", "tp"), None)
    return jax.shard_map(shards, mesh=mesh, in_specs=in_specs, out_specs=out_specs, check_vma=False)
```

```python
import jax
import jax.numpy as jnp
from jax import lax
from jax.experimental import pallas as pl
from jax.experimental.pallas import tpu as pltpu
from jax.sharding import PartitionSpec as P

MESH = pl.DeviceIdType.MESH
RESIDUAL = 1.6817928
NX = 4
NZ = 4
NSP = 16
NTP = 8
CAP = 5
LB = 8
NT = 4
F32 = jnp.float32
BF16 = jnp.bfloat16


def layer_norm(v, gain, bias):
    mean = jnp.mean(v, axis=-1, keepdims=True)
    cent = v - mean
    var = jnp.mean(cent * cent, axis=-1, keepdims=True)
    return cent * lax.rsqrt(var + 1e-05) * gain + bias


def one_hot(cond):
    return jnp.where(cond, 1.0, 0.0).astype(BF16)


def body(
    stream_h, og_h, ig_h, va_h, cw_h, ow_h, doc_h, rt_h, rw_h, ng_h, nb_h, wg_h, wu_h, wd_h,
    out_ref,
    stream, og, ig, va, cw, ow, doc, rt, rw, ng, nb, wg, wu, wd,
    ext, halo, term, terms, mx, tr, acc, normed, snd, rcv, xb, hb, pf, pb, rd, q, rab, snd2, ret,
    rt_o, rw_o, normed_o, snd_o, rcv_o, snd2_o, ret_o, part_o, part, turn,
    lsem, h_s, h_r, i_s, i_r, a_s, a_r, b_s, b_r, g_s, g_r, p_s, p_r, d_s, d_r, q_s, q_r, e_s, e_r,
    o_s, o_r, c_s, c_r, f_s, f_r,
):
    sp = lax.axis_index("sp")
    tp = lax.axis_index("tp")
    z, x = sp // NX, sp % NX
    y, c = tp // 2, tp % 2
    width = og.shape[1]
    length = og.shape[0]
    model = stream.shape[1]
    rows = stream.shape[0]
    hidden = wg.shape[1]
    blk = NSP * CAP
    tile = model // NT
    half = model // 2
    per = NT // 2

    def sp_at(d):
        return ((z + d // NX) % NZ) * NX + (x + d % NX) % NX

    def sp_back(d):
        return ((z - d // NX + NZ) % NZ) * NX + (x - d % NX + NX) % NX

    def tp_at(o):
        return ((y + o // 2) % 4) * 2 + (c + o % 2) % 2

    def tp_from(o):
        return ((y - o // 2 + 4) % 4) * 2 + (c - o % 2 + 2) % 2

    def remote(src, dst, ss, rs, dev):
        return pltpu.make_async_remote_copy(
            src_ref=src, dst_ref=dst, send_sem=ss, recv_sem=rs, device_id=dev, device_id_type=MESH
        )

    def whole(ref, sem):
        remote(ref, ref, sem, sem, (sp, tp)).wait_recv()

    barrier = pltpu.get_barrier_semaphore()
    for d in range(1, NSP):
        pl.semaphore_signal(barrier, inc=1, device_id=(sp_at(d), tp), device_id_type=MESH)
    for o in range(1, NTP):
        pl.semaphore_signal(barrier, inc=1, device_id=(sp, tp_at(o)), device_id_type=MESH)

    nxt = (sp + 1) % NSP

    local = [
        pltpu.make_async_copy(src, dst, lsem.at[i])
        for i, (src, dst) in enumerate(
            [
                (ig_h, ig), (va_h, va), (cw_h, cw), (doc_h, doc), (og_h, og), (rt_h, rt), (rw_h, rw),
                (stream_h, stream), (ng_h, ng), (nb_h, nb), (ow_h, ow),
                (wg_h.at[0], wg), (wu_h.at[0], wu), (wd_h.at[0], wd),
            ]
        )
    ]
    for copy in local[:10]:
        copy.start()

    for i in range(4):
        local[i].wait()
    ext[0:8, :width] = jnp.zeros((8, width), F32)
    ext[0:8, width:] = jnp.full((8, 128), -1.0, F32)
    ext[8:8 + length, :width] = ig[...].astype(F32) * va[...].astype(F32)
    ext[8:8 + length, width:] = jnp.transpose(jnp.broadcast_to(doc[...].astype(F32), (128, length)))
    local[4].wait()
    local[10].start()
    pl.semaphore_wait(barrier, NSP + NTP - 2)
    halo_copy = remote(ext.at[pl.ds(length, 8), :], halo, h_s, h_r, (nxt, tp))
    halo_copy.start()
    far = (sp, ((y + 2) % 4) * 2 + c)
    local[5].wait()
    local[6].wait()
    far_copies = [
        remote(src, dst, o_s.at[i], o_r.at[i], far)
        for i, (src, dst) in enumerate([
            (rt, rt_o), (rw, rw_o),
            (normed.at[:, pl.ds(0, half)], normed_o.at[:, pl.ds(0, half)]),
            (normed.at[:, pl.ds(half, half)], normed_o.at[:, pl.ds(half, half)]),
            (part_o.at[:, pl.ds(0, half)], part.at[:, pl.ds(0, half)]),
            (part_o.at[:, pl.ds(half, half)], part.at[:, pl.ds(half, half)]),
        ])
    ]
    far_copies[0].start()
    far_copies[1].start()

    def convolved(r0, n):
        d0 = ext[8 + r0:8 + r0 + n, width:]
        keep1 = jnp.where(ext[7 + r0:7 + r0 + n, width:] == d0, 1.0, 0.0)
        keep2 = jnp.where(ext[6 + r0:6 + r0 + n, width:] == d0, 1.0, 0.0)
        keep1 = jnp.concatenate([keep1] * (width // 128), axis=1)
        keep2 = jnp.concatenate([keep2] * (width // 128), axis=1)
        return (
            cw[0:1, :] * ext[6 + r0:6 + r0 + n, :width] * keep2
            + cw[1:2, :] * ext[7 + r0:7 + r0 + n, :width] * keep1
            + cw[2:3, :] * ext[8 + r0:8 + r0 + n, :width]
        )

    for t in range(NTP):
        mx[t] = (og[t * rows:(t + 1) * rows, :].astype(F32) * convolved(t * rows, rows)).astype(BF16)
    a_copies = [
        remote(mx.at[tp_at(o)], tr.at[o], a_s, a_r.at[o], (sp, tp_at(o))) for o in range(1, NTP)
    ]
    for o in (4, 5, 2, 3, 6, 7, 1):
        a_copies[o - 1].start()
    for copy in local[11:]:
        copy.start()

    lanes = lax.broadcasted_iota(jnp.int32, (NSP, rows), 0)
    upper = one_hot(
        lax.broadcasted_iota(jnp.int32, (rows, rows), 0) < lax.broadcasted_iota(jnp.int32, (rows, rows), 1)
    )
    slots = lax.broadcasted_iota(jnp.int32, (blk, rows), 0)
    eye = lax.broadcasted_iota(jnp.int32, (rows, rows), 0) == lax.broadcasted_iota(jnp.int32, (rows, rows), 1)

    def placed(table):
        rel = []
        for k in range(2):
            e = table[k:k + 1, :]
            rel.append((((e >> 2) + (NZ - z)) & 3) * NX + (((e & 3) + (NX - x)) & 3))
        hot = [jnp.where(lanes == r, 1.0, 0.0) for r in rel]
        prefix = jnp.dot((hot[0] + hot[1]).astype(BF16), upper, preferred_element_type=F32)
        place = []
        for k in range(2):
            rank = jnp.sum(prefix * hot[k], axis=0, keepdims=True)
            slot = rel[k] * CAP + rank.astype(jnp.int32)
            place.append(jnp.where(slots == slot, 1.0, 0.0))
        return place

    def weights(table):
        return [jnp.sum(jnp.where(eye, table[k:k + 1, :], 0.0), axis=1, keepdims=True) for k in range(2)]

    place = placed(rt)

    for i in range(7, 11):
        local[i].wait()

    def project(lhs, t):
        start = pl.multiple_of(t * width, width)
        return jnp.dot(lhs, ow[pl.ds(start, width), :], preferred_element_type=F32)

    acc[...] = RESIDUAL * stream[...].astype(F32) + project(mx[tp], tp)
    def edge_rows():
        halo_copy.wait_recv()
        ext[0:8, :width] = halo[:, :width]
        ext[0:8, width:] = jnp.where(sp == 0, -1.0, halo[:, width:])
        fixed = (og[0:16, :].astype(F32) * convolved(0, 16)).astype(BF16)
        term[...] = project(fixed, tp)[0:2, :]

        @pl.when(tp != 0)
        def _():
            remote(term, terms.at[tp], i_s, i_r, (sp, 0)).start()

    edge_rows()
    for o in (1, 2, 3, 6, 7, 4, 5):
        a_copies[o - 1].wait_recv()
        acc[...] += project(tr[o], tp_from(o))
    @pl.when(tp == 0)
    def _():
        whole(terms.at[pl.ds(1, NTP - 1)], i_r)
        total = term[...]
        for t in range(1, NTP):
            total += terms[t]
        acc[0:2, :] = RESIDUAL * stream[0:2, :].astype(F32) + total

    normed[...] = layer_norm(acc[...], ng[0:1, :], nb[0:1, :]).astype(BF16)

    far_copies[2].start()
    far_copies[3].start()

    def fold(rows_f32, dst, h):
        for b in range(LB):
            turn[pl.ds(b, blk, stride=LB), :] = rows_f32[:, b * 128:(b + 1) * 128]
        dst[h] = turn[...].reshape(NSP, CAP * LB, 128).astype(BF16)

    def unfold(src, h):
        turn[...] = src[h].astype(F32).reshape(blk * LB, 128)
        return jnp.concatenate(
            [turn[pl.ds(b, blk, stride=LB), :].astype(BF16) for b in range(LB)], axis=1
        )

    def pack(place, src, dst, h):
        both = (place[0] + place[1]).astype(BF16)
        fold(jnp.dot(both, src[:, h * half:(h + 1) * half], preferred_element_type=F32), dst, h)

    def halves(src, dst, ss, rs, to):
        return [
            {
                d: remote(src.at[h, d], dst.at[h, d], ss, rs.at[h], (to(d), tp))
                for d in range(1, NSP)
            }
            for h in range(2)
        ]

    sp_order = (10, 9, 11, 6, 14, 5, 7, 13, 15, 2, 8, 1, 3, 4, 12)
    b_copies = halves(snd, rcv, b_s, b_r, sp_at)
    c_copies = halves(snd_o, rcv_o, c_s, c_r, sp_at)
    e_copies = halves(snd2, ret, e_s, e_r, sp_back)
    f_copies = halves(snd2_o, ret_o, f_s, f_r, sp_back)

    def start_all(copies):
        for d in sp_order:
            copies[d].start()

    def arrive_all(dst, rs, h):
        whole(dst.at[h, pl.ds(1, NSP - 1)], rs.at[h])

    for h in range(2):
        pack(place, normed, snd, h)
        start_all(b_copies[h])
        rcv[h, 0] = snd[h, 0]
    far_copies[0].wait_recv()
    far_copies[1].wait_recv()
    place_o = placed(rt_o)
    def side_of(row):
        return (1 - 2 * c) * (1 - 2 * (row // 3))

    side = side_of(y)
    above, below = (y + 1) % 4, (y + 3) % 4
    first_above = side_of(above) == -1
    first_below = side_of(below) == 1
    toward = [(sp, ((y + side + 4) % 4) * 2 + c), (sp, ((y - side + 4) % 4) * 2 + c)]
    mate = (sp, y * 2 + 1 - c)
    position = {0: 0, 4: 1, 3: 2, 7: 3, 1: 4, 5: 5, 2: 6, 6: 7}

    def settle(src, j, h):
        r0 = position[j] * blk
        xb[h, r0:r0 + blk, :] = unfold(src, h)

    def block(j, h):
        return xb.at[h, pl.ds(position[j] * blk, blk), :]

    def neighbour(row, is_first, h):
        k = jnp.where(is_first, 0, 1)
        rows_at = pl.multiple_of((position[1] + k * (position[2] - position[1])) * blk, blk)
        return remote(
            block(0, h), xb.at[h, pl.ds(rows_at, blk), :], g_s, g_r.at[2 * k + h], (sp, row * 2 + c)
        )

    to_near = [
        (first_above, [neighbour(above, first_above, h) for h in range(2)]),
        (first_below, [neighbour(below, first_below, h) for h in range(2)]),
    ]

    def from_near(j, h):
        remote(block(0, h), block(j, h), g_s, g_r.at[2 * (j - 1) + h], mate).wait_recv()

    pair = [
        [remote(block(j, h), block(4 + j, h), p_s, p_r.at[j], mate) for h in range(2)]
        for j in range(4)
    ]

    def gather_half(h):
        arrive_all(rcv, b_r, h)
        settle(rcv, 0, h)
        pair[0][h].start()
        for is_first, copies in to_near:
            @pl.when(is_first)
            def _():
                copies[h].start()

    def far_dispatch():
        for h in range(2):
            far_copies[2 + h].wait_recv()
            pack(place_o, normed_o, snd_o, h)
            start_all(c_copies[h])
            rcv_o[h, 0] = snd_o[h, 0]

    pl.when(tp == 0)(far_dispatch)
    gather_half(0)
    pl.when((tp != 0) & (tp != 4))(far_dispatch)
    gather_half(1)
    pl.when(tp == 4)(far_dispatch)

    def gate_up(j, beside={}):
        r0 = position[j] * blk
        lo, hi = (xb.at[h, pl.ds(r0, 2 * blk), :] for h in range(2))
        for i, c0 in enumerate(range(0, hidden, 256)):
            cols = slice(c0, min(c0 + 256, hidden))
            start = beside[i]() if i in beside else None
            gate, upp = [
                jnp.dot(lo[...], w[:half, cols], preferred_element_type=F32)
                + jnp.dot(hi[...], w[half:, cols], preferred_element_type=F32)
                for w in (wg, wu)
            ]
            hb[:, cols] = (gate / (1.0 + jnp.exp(-gate)) * upp).astype(BF16)
            if start:
                start()

    def d2d(j, n):
        view = (n, pl.ds(j * blk, blk))
        return remote(pb.at[view], rd.at[view], d_s, d_r.at[2 * j + n // per], mate)

    def d2d_in(j, h):
        whole(rd.at[pl.ds(h * per, per), pl.ds(j * blk, blk)], d_r.at[2 * j + h])

    def pair_in(j):
        whole(xb.at[:, pl.ds(position[4 + j] * blk, blk)], p_r.at[j])

    def down_tiles(j, tiles):
        for n in tiles:
            part = jnp.dot(hb[...], wd[:, n * tile:(n + 1) * tile], preferred_element_type=F32)
            pf[n, j * blk:(j + 1) * blk, :] = part[:blk]
            pb[n, j * blk:(j + 1) * blk, :] = part[blk:].astype(BF16)
        for n in tiles:
            d2d(j, n).start()

    behind = (1 + side) // 2

    def send(j, n):
        k = behind if j == 1 else 1 - behind
        return remote(q.at[j - 1, n], rab.at[k, n], q_s, q_r.at[2 * k + n // per], toward[j - 1])

    def summed(j, n):
        return pf[n, j * blk:(j + 1) * blk, :] + rd[n, j * blk:(j + 1) * blk, :].astype(F32)

    def finish(j, h):
        d2d_in(j, h)
        tiles = range(h * per, (h + 1) * per)
        for n in tiles:
            q[j - 1, n] = summed(j, n).astype(BF16)
        return lambda: [send(j, n).start() for n in tiles]

    def far_total(h):
        d2d_in(3, h)
        fold(jnp.concatenate([summed(3, n) for n in range(h * per, (h + 1) * per)], axis=1), snd2_o, h)
        ret_o[h, 0] = snd2_o[h, 0]
        return lambda: start_all(f_copies[h])

    def down_pass(j):
        down_tiles(j, range(per))
        down_tiles(j, range(per, NT))

    def other_side():
        for h in range(2):
            from_near(2, h)
            pair[2][h].start()

    local[11].wait()
    local[12].wait()
    local[13].wait()
    @pl.when(y != 0)
    def _():
        pair_in(0)
        gate_up(0)

    for is_first, copies in to_near:
        @pl.when(jnp.logical_not(is_first))
        def _():
            copies[0].start()
            copies[1].start()
    from_near(1, 0)
    pair[1][0].start()
    from_near(1, 1)
    pair[1][1].start()
    @pl.when(y != 0)
    def _():
        down_tiles(0, range(NT))

    for h in range(2):
        arrive_all(rcv_o, c_r, h)
        settle(rcv_o, 3, h)
        pair[3][h].start()
    pair_in(1)
    gate_up(1)
    down_pass(1)
    pair_in(3)
    gate_up(3, {2: other_side, 3: lambda: finish(1, 0)})
    down_tiles(3, range(per))
    finish(1, 1)()
    down_tiles(3, range(per, NT))
    pair_in(2)
    gate_up(2)
    down_pass(2)
    @pl.when(y == 0)
    def _():
        pair_in(0)
        gate_up(0, {
            0: lambda: far_total(0), 1: lambda: finish(2, 0), 2: lambda: far_total(1), 3: lambda: finish(2, 1),
        })
        down_pass(0)

    @pl.when(y != 0)
    def _():
        for h in range(2):
            far_total(h)()
            finish(2, h)()

    def picked(place, weight, src, h):
        came = unfold(src, h)
        routed = [
            weight[k] * lax.dot_general(
                place[k].astype(BF16), came, (((0,), (0,)), ((), ())), preferred_element_type=F32
            )
            for k in range(2)
        ]
        return routed[0] + routed[1]

    weight_o = weights(rw_o)
    weight = weights(rw)

    def own_total(h):
        d2d_in(0, h)
        for k in range(2):
            whole(rab.at[k, pl.ds(h * per, per)], q_r.at[2 * k + h])
        sums = [
            summed(0, n) + rab[0, n].astype(F32) + rab[1, n].astype(F32)
            for n in range(h * per, (h + 1) * per)
        ]
        fold(jnp.concatenate(sums, axis=1), snd2, h)
        start_all(e_copies[h])
        ret[h, 0] = snd2[h, 0]

    own_total(0)
    own_total(1)
    for h in range(2):
        arrive_all(ret_o, f_r, h)
        part_o[:, h * half:(h + 1) * half] = picked(place_o, weight_o, ret_o, h).astype(BF16)
        far_copies[4 + h].start()
    halo_copy.wait_send()

    @pl.when(tp != 0)
    def _():
        remote(term, terms.at[tp], i_s, i_r, (sp, 0)).wait_send()

    for copy in far_copies[:4]:
        copy.wait_send()
    whole(mx.at[pl.ds(1, NTP - 1)], a_s)
    for src, ss in ((snd, b_s), (snd_o, c_s), (snd2_o, f_s)):
        whole(src.at[:, pl.ds(1, NSP - 1)], ss)
    whole(xb.at[0, pl.ds(0, 4 * blk)], g_s)
    whole(xb.at[0], p_s)
    whole(pb, d_s)
    whole(q, q_s)
    for h in range(2):
        cols = slice(h * half, (h + 1) * half)
        arrive_all(ret, e_r, h)
        acc[:, cols] = RESIDUAL * normed[:, cols].astype(F32) + picked(place, weight, ret, h)
    far_copies[4].wait_recv()
    far_copies[5].wait_recv()
    acc[...] += part[...].astype(F32)
    out_ref[...] = layer_norm(acc[...], ng[1:2, :], nb[1:2, :]).astype(BF16)

    far_copies[4].wait_send()
    far_copies[5].wait_send()
    whole(snd2.at[:, pl.ds(1, NSP - 1)], e_s)


def shards(stream, out_gate, in_gate, values, conv_weight, out_weight, doc_ids, routes, route_weight,
           norm_gain, norm_bias, expert_gate, expert_up, expert_down):
    length, width = out_gate.shape
    rows, model = stream.shape
    hidden = expert_gate.shape[2]
    blk = NSP * CAP
    any_spec = pl.BlockSpec(memory_space=pltpu.HBM)
    dma = pltpu.SemaphoreType.DMA
    scratch = [
        pltpu.VMEM((rows, model), BF16),
        pltpu.VMEM((length, width), BF16),
        pltpu.VMEM((length, width), BF16),
        pltpu.VMEM((length, width), BF16),
        pltpu.VMEM((3, width), F32),
        pltpu.VMEM((model, model), BF16),
        pltpu.VMEM((1, length), jnp.int32),
        pltpu.VMEM((2, rows), jnp.int32),
        pltpu.VMEM((2, rows), F32),
        pltpu.VMEM((2, model), F32),
        pltpu.VMEM((2, model), F32),
        pltpu.VMEM((model, hidden), BF16),
        pltpu.VMEM((model, hidden), BF16),
        pltpu.VMEM((hidden, model), BF16),
        pltpu.VMEM((8 + length, width + 128), F32),
        pltpu.VMEM((8, width + 128), F32),
        pltpu.VMEM((2, model), F32),
        pltpu.VMEM((NTP, 2, model), F32),
        pltpu.VMEM((NTP, rows, width), BF16),
        pltpu.VMEM((NTP, rows, width), BF16),
        pltpu.VMEM((rows, model), F32),
        pltpu.VMEM((rows, model), BF16),
        pltpu.VMEM((2, NSP, CAP * LB, 128), BF16),
        pltpu.VMEM((2, NSP, CAP * LB, 128), BF16),
        pltpu.VMEM((2, 8 * blk, model // 2), BF16),
        pltpu.VMEM((2 * blk, hidden), BF16),
        pltpu.VMEM((NT, 4 * blk, model // NT), F32),
        pltpu.VMEM((NT, 4 * blk, model // NT), BF16),
        pltpu.VMEM((NT, 4 * blk, model // NT), BF16),
        pltpu.VMEM((2, NT, blk, model // NT), BF16),
        pltpu.VMEM((2, NT, blk, model // NT), BF16),
        pltpu.VMEM((2, NSP, CAP * LB, 128), BF16),
        pltpu.VMEM((2, NSP, CAP * LB, 128), BF16),
        pltpu.VMEM((2, rows), jnp.int32),
        pltpu.VMEM((2, rows), F32),
        pltpu.VMEM((rows, model), BF16),
        pltpu.VMEM((2, NSP, CAP * LB, 128), BF16),
        pltpu.VMEM((2, NSP, CAP * LB, 128), BF16),
        pltpu.VMEM((2, NSP, CAP * LB, 128), BF16),
        pltpu.VMEM((2, NSP, CAP * LB, 128), BF16),
        pltpu.VMEM((rows, model), BF16),
        pltpu.VMEM((rows, model), BF16),
        pltpu.VMEM((blk * LB, 128), F32),
        dma((14,)), dma, dma, dma, dma, dma, dma((NTP,)), dma, dma((2,)),
        dma, dma((4,)), dma, dma((4,)), dma, dma((8,)),
        dma, dma((4,)), dma, dma((2,)),
        dma((6,)), dma((6,)), dma, dma((2,)), dma, dma((2,)),
    ]
    return pl.pallas_call(
        body,
        out_shape=jax.ShapeDtypeStruct((rows, model), BF16),
        in_specs=[any_spec] * 14,
        out_specs=pl.BlockSpec(memory_space=pltpu.VMEM),
        scratch_shapes=scratch,
        compiler_params=pltpu.CompilerParams(
            collective_id=0, has_side_effects=True, vmem_limit_bytes=48 * 1024 * 1024
        ),
        name="layer",
    )(*[pltpu.with_memory_space_constraint(v, pltpu.HBM) for v in (
        stream, out_gate, in_gate, values, conv_weight, out_weight, doc_ids.reshape(1, -1),
        routes.T, route_weight.T, norm_gain, norm_bias, expert_gate, expert_up, expert_down,
    )])


def solution(mesh):
    in_specs = (
        P(("sp", "tp"), None),
        P("sp", "tp"),
        P("sp", "tp"),
        P("sp", "tp"),
        P(None, "tp"),
        P(),
        P("sp"),
        P(("sp", "tp"), None),
        P(("sp", "tp"), None),
        P(),
        P(),
        P("sp", None, "tp"),
        P("sp", None, "tp"),
        P("sp", "tp", None),
    )
    out_specs = P(("sp", "tp"), None)
    return jax.shard_map(shards, mesh=mesh, in_specs=in_specs, out_specs=out_specs, check_vma=False)
```

```python
import jax
import jax.numpy as jnp
from jax import lax
from jax.experimental import pallas as pl
from jax.experimental.pallas import tpu as pltpu
from jax.sharding import PartitionSpec as P

MESH = pl.DeviceIdType.MESH
RESIDUAL = 1.6817928
NX = 4
NZ = 4
NSP = 16
NTP = 8
CAP = 5
LB = 8
NT = 4
F32 = jnp.float32
BF16 = jnp.bfloat16


def layer_norm(v, gain, bias):
    mean = jnp.mean(v, axis=-1, keepdims=True)
    cent = v - mean
    var = jnp.mean(cent * cent, axis=-1, keepdims=True)
    return cent * lax.rsqrt(var + 1e-05) * gain + bias


def one_hot(cond):
    return jnp.where(cond, 1.0, 0.0).astype(BF16)


def body(
    stream_h, og_h, ig_h, va_h, cw_h, ow_h, doc_h, rt_h, rw_h, ng_h, nb_h, wg_h, wu_h, wd_h,
    out_ref,
    stream, og, ig, va, cw, ow, doc, rt, rw, ng, nb, wg, wu, wd,
    ext, halo, term, terms, mx, tr, acc, normed, snd, rcv, xb, hb, pf, pb, rd, q, rab, snd2, ret,
    rt_o, rw_o, normed_o, snd_o, rcv_o, snd2_o, ret_o, part_o, part, turn,
    lsem, h_s, h_r, i_s, i_r, a_s, a_r, b_s, b_r, g_s, g_r, p_s, p_r, d_s, d_r, q_s, q_r, e_s, e_r,
    o_s, o_r, c_s, c_r, f_s, f_r,
):
    sp = lax.axis_index("sp")
    tp = lax.axis_index("tp")
    z, x = sp // NX, sp % NX
    y, c = tp // 2, tp % 2
    width = og.shape[1]
    length = og.shape[0]
    model = stream.shape[1]
    rows = stream.shape[0]
    hidden = wg.shape[1]
    blk = NSP * CAP
    tile = model // NT
    half = model // 2
    per = NT // 2

    def sp_at(d):
        return ((z + d // NX) % NZ) * NX + (x + d % NX) % NX

    def sp_back(d):
        return ((z - d // NX + NZ) % NZ) * NX + (x - d % NX + NX) % NX

    def tp_at(o):
        return ((y + o // 2) % 4) * 2 + (c + o % 2) % 2

    def tp_from(o):
        return ((y - o // 2 + 4) % 4) * 2 + (c - o % 2 + 2) % 2

    def remote(src, dst, ss, rs, dev):
        return pltpu.make_async_remote_copy(
            src_ref=src, dst_ref=dst, send_sem=ss, recv_sem=rs, device_id=dev, device_id_type=MESH
        )

    def whole(ref, sem):
        remote(ref, ref, sem, sem, (sp, tp)).wait_recv()

    barrier = pltpu.get_barrier_semaphore()
    for d in range(1, NSP):
        pl.semaphore_signal(barrier, inc=1, device_id=(sp_at(d), tp), device_id_type=MESH)
    for o in range(1, NTP):
        pl.semaphore_signal(barrier, inc=1, device_id=(sp, tp_at(o)), device_id_type=MESH)

    nxt = (sp + 1) % NSP

    local = [
        pltpu.make_async_copy(src, dst, lsem.at[i])
        for i, (src, dst) in enumerate(
            [
                (ig_h, ig), (va_h, va), (cw_h, cw), (doc_h, doc), (og_h, og), (rt_h, rt), (rw_h, rw),
                (stream_h, stream), (ng_h, ng), (nb_h, nb), (ow_h, ow),
                (wg_h.at[0], wg), (wu_h.at[0], wu), (wd_h.at[0], wd),
            ]
        )
    ]
    for copy in local[:10]:
        copy.start()

    for i in range(4):
        local[i].wait()
    ext[0:8, :width] = jnp.zeros((8, width), F32)
    ext[0:8, width:] = jnp.full((8, 128), -1.0, F32)
    ext[8:8 + length, :width] = ig[...].astype(F32) * va[...].astype(F32)
    ext[8:8 + length, width:] = jnp.transpose(jnp.broadcast_to(doc[...].astype(F32), (128, length)))
    local[4].wait()
    local[10].start()
    pl.semaphore_wait(barrier, NSP + NTP - 2)
    halo_copy = remote(ext.at[pl.ds(length, 8), :], halo, h_s, h_r, (nxt, tp))
    halo_copy.start()
    far = (sp, ((y + 2) % 4) * 2 + c)
    local[5].wait()
    local[6].wait()
    far_copies = [
        remote(src, dst, o_s.at[i], o_r.at[i], far)
        for i, (src, dst) in enumerate([
            (rt, rt_o), (rw, rw_o),
            (normed.at[:, pl.ds(0, half)], normed_o.at[:, pl.ds(0, half)]),
            (normed.at[:, pl.ds(half, half)], normed_o.at[:, pl.ds(half, half)]),
            (part_o.at[:, pl.ds(0, half)], part.at[:, pl.ds(0, half)]),
            (part_o.at[:, pl.ds(half, half)], part.at[:, pl.ds(half, half)]),
        ])
    ]
    far_copies[0].start()
    far_copies[1].start()

    def convolved(r0, n):
        d0 = ext[8 + r0:8 + r0 + n, width:]
        keep1 = jnp.where(ext[7 + r0:7 + r0 + n, width:] == d0, 1.0, 0.0)
        keep2 = jnp.where(ext[6 + r0:6 + r0 + n, width:] == d0, 1.0, 0.0)
        keep1 = jnp.concatenate([keep1] * (width // 128), axis=1)
        keep2 = jnp.concatenate([keep2] * (width // 128), axis=1)
        return (
            cw[0:1, :] * ext[6 + r0:6 + r0 + n, :width] * keep2
            + cw[1:2, :] * ext[7 + r0:7 + r0 + n, :width] * keep1
            + cw[2:3, :] * ext[8 + r0:8 + r0 + n, :width]
        )

    for t in range(NTP):
        mx[t] = (og[t * rows:(t + 1) * rows, :].astype(F32) * convolved(t * rows, rows)).astype(BF16)
    a_copies = [
        remote(mx.at[tp_at(o)], tr.at[o], a_s, a_r.at[o], (sp, tp_at(o))) for o in range(1, NTP)
    ]
    for o in (4, 5, 2, 3, 6, 7, 1):
        a_copies[o - 1].start()
    for copy in local[11:]:
        copy.start()

    lanes = lax.broadcasted_iota(jnp.int32, (NSP, rows), 0)
    upper = one_hot(
        lax.broadcasted_iota(jnp.int32, (rows, rows), 0) < lax.broadcasted_iota(jnp.int32, (rows, rows), 1)
    )
    slots = lax.broadcasted_iota(jnp.int32, (blk, rows), 0)
    eye = lax.broadcasted_iota(jnp.int32, (rows, rows), 0) == lax.broadcasted_iota(jnp.int32, (rows, rows), 1)

    def placed(table):
        rel = []
        for k in range(2):
            e = table[k:k + 1, :]
            rel.append((((e >> 2) + (NZ - z)) & 3) * NX + (((e & 3) + (NX - x)) & 3))
        hot = [jnp.where(lanes == r, 1.0, 0.0) for r in rel]
        prefix = jnp.dot((hot[0] + hot[1]).astype(BF16), upper, preferred_element_type=F32)
        place = []
        for k in range(2):
            rank = jnp.sum(prefix * hot[k], axis=0, keepdims=True)
            slot = rel[k] * CAP + rank.astype(jnp.int32)
            place.append(jnp.where(slots == slot, 1.0, 0.0))
        return place

    def weights(table):
        return [jnp.sum(jnp.where(eye, table[k:k + 1, :], 0.0), axis=1, keepdims=True) for k in range(2)]

    place = placed(rt)

    for i in range(7, 11):
        local[i].wait()

    def project(lhs, t):
        start = pl.multiple_of(t * width, width)
        return jnp.dot(lhs, ow[pl.ds(start, width), :], preferred_element_type=F32)

    acc[...] = RESIDUAL * stream[...].astype(F32) + project(mx[tp], tp)
    def edge_rows():
        halo_copy.wait_recv()
        ext[0:8, :width] = halo[:, :width]
        ext[0:8, width:] = jnp.where(sp == 0, -1.0, halo[:, width:])
        fixed = (og[0:16, :].astype(F32) * convolved(0, 16)).astype(BF16)
        term[...] = project(fixed, tp)[0:2, :]

        @pl.when(tp != 0)
        def _():
            remote(term, terms.at[tp], i_s, i_r, (sp, 0)).start()

    pl.when(x != 0)(edge_rows)
    for o in (1, 2, 3, 6, 7, 4, 5):
        a_copies[o - 1].wait_recv()
        acc[...] += project(tr[o], tp_from(o))
        if o == 3:
            pl.when(x == 0)(edge_rows)
    @pl.when(tp == 0)
    def _():
        whole(terms.at[pl.ds(1, NTP - 1)], i_r)
        total = term[...]
        for t in range(1, NTP):
            total += terms[t]
        acc[0:2, :] = RESIDUAL * stream[0:2, :].astype(F32) + total

    normed[...] = layer_norm(acc[...], ng[0:1, :], nb[0:1, :]).astype(BF16)

    far_copies[2].start()
    far_copies[3].start()

    def fold(rows_f32, dst, h):
        for b in range(LB):
            turn[pl.ds(b, blk, stride=LB), :] = rows_f32[:, b * 128:(b + 1) * 128]
        dst[h] = turn[...].reshape(NSP, CAP * LB, 128).astype(BF16)

    def unfold(src, h):
        turn[...] = src[h].astype(F32).reshape(blk * LB, 128)
        return jnp.concatenate(
            [turn[pl.ds(b, blk, stride=LB), :].astype(BF16) for b in range(LB)], axis=1
        )

    def pack(place, src, dst, h):
        both = (place[0] + place[1]).astype(BF16)
        fold(jnp.dot(both, src[:, h * half:(h + 1) * half], preferred_element_type=F32), dst, h)

    def halves(src, dst, ss, rs, to):
        return [
            {
                d: remote(src.at[h, d], dst.at[h, d], ss, rs.at[h], (to(d), tp))
                for d in range(1, NSP)
            }
            for h in range(2)
        ]

    sp_order = (10, 9, 11, 6, 14, 5, 7, 13, 15, 2, 8, 1, 3, 4, 12)
    b_copies = halves(snd, rcv, b_s, b_r, sp_at)
    c_copies = halves(snd_o, rcv_o, c_s, c_r, sp_at)
    e_copies = halves(snd2, ret, e_s, e_r, sp_back)
    f_copies = halves(snd2_o, ret_o, f_s, f_r, sp_back)

    def start_all(copies):
        for d in sp_order:
            copies[d].start()

    def arrive_all(dst, rs, h):
        whole(dst.at[h, pl.ds(1, NSP - 1)], rs.at[h])

    for h in range(2):
        pack(place, normed, snd, h)
        start_all(b_copies[h])
        rcv[h, 0] = snd[h, 0]
    far_copies[0].wait_recv()
    far_copies[1].wait_recv()
    place_o = placed(rt_o)
    def side_of(row):
        return (1 - 2 * c) * (2 * (((row + 1) % 4) // 2) - 1)

    side = side_of(y)
    above, below = (y + 1) % 4, (y + 3) % 4
    first_above = side_of(above) == -1
    first_below = side_of(below) == 1
    toward = [(sp, ((y + side + 4) % 4) * 2 + c), (sp, ((y - side + 4) % 4) * 2 + c)]
    mate = (sp, y * 2 + 1 - c)
    position = {0: 0, 4: 1, 3: 2, 7: 3, 1: 4, 5: 5, 2: 6, 6: 7}

    def settle(src, j, h):
        r0 = position[j] * blk
        xb[h, r0:r0 + blk, :] = unfold(src, h)

    def block(j, h):
        return xb.at[h, pl.ds(position[j] * blk, blk), :]

    def neighbour(row, is_first, h):
        k = jnp.where(is_first, 0, 1)
        rows_at = pl.multiple_of((position[1] + k * (position[2] - position[1])) * blk, blk)
        return remote(
            block(0, h), xb.at[h, pl.ds(rows_at, blk), :], g_s, g_r.at[2 * k + h], (sp, row * 2 + c)
        )

    to_near = [
        (first_above, [neighbour(above, first_above, h) for h in range(2)]),
        (first_below, [neighbour(below, first_below, h) for h in range(2)]),
    ]

    def from_near(j, h):
        remote(block(0, h), block(j, h), g_s, g_r.at[2 * (j - 1) + h], mate).wait_recv()

    pair = [
        [remote(block(j, h), block(4 + j, h), p_s, p_r.at[j], mate) for h in range(2)]
        for j in range(4)
    ]

    def gather_half(h):
        arrive_all(rcv, b_r, h)
        settle(rcv, 0, h)
        pair[0][h].start()
        for is_first, copies in to_near:
            @pl.when(is_first)
            def _():
                copies[h].start()

    def far_dispatch():
        for h in range(2):
            far_copies[2 + h].wait_recv()
            pack(place_o, normed_o, snd_o, h)
            start_all(c_copies[h])
            rcv_o[h, 0] = snd_o[h, 0]

    pl.when(tp == 0)(far_dispatch)
    gather_half(0)
    pl.when((tp != 0) & (tp != 4))(far_dispatch)
    gather_half(1)
    pl.when(tp == 4)(far_dispatch)

    def gate_up(j, beside={}):
        r0 = position[j] * blk
        lo, hi = (xb.at[h, pl.ds(r0, 2 * blk), :] for h in range(2))
        for i, c0 in enumerate(range(0, hidden, 256)):
            cols = slice(c0, min(c0 + 256, hidden))
            start = beside[i]() if i in beside else None
            gate, upp = [
                jnp.dot(lo[...], w[:half, cols], preferred_element_type=F32)
                + jnp.dot(hi[...], w[half:, cols], preferred_element_type=F32)
                for w in (wg, wu)
            ]
            hb[:, cols] = (gate / (1.0 + jnp.exp(-gate)) * upp).astype(BF16)
            if start:
                start()

    def d2d(j, n):
        view = (n, pl.ds(j * blk, blk))
        return remote(pb.at[view], rd.at[view], d_s, d_r.at[2 * j + n // per], mate)

    def d2d_in(j, h):
        whole(rd.at[pl.ds(h * per, per), pl.ds(j * blk, blk)], d_r.at[2 * j + h])

    def pair_in(j):
        whole(xb.at[:, pl.ds(position[4 + j] * blk, blk)], p_r.at[j])

    def down_tiles(j, tiles):
        for n in tiles:
            part = jnp.dot(hb[...], wd[:, n * tile:(n + 1) * tile], preferred_element_type=F32)
            pf[n, j * blk:(j + 1) * blk, :] = part[:blk]
            pb[n, j * blk:(j + 1) * blk, :] = part[blk:].astype(BF16)
        for n in tiles:
            d2d(j, n).start()

    behind = (1 + side) // 2

    def send(j, n):
        k = behind if j == 1 else 1 - behind
        return remote(q.at[j - 1, n], rab.at[k, n], q_s, q_r.at[2 * k + n // per], toward[j - 1])

    def summed(j, n):
        return pf[n, j * blk:(j + 1) * blk, :] + rd[n, j * blk:(j + 1) * blk, :].astype(F32)

    def finish(j, h):
        d2d_in(j, h)
        tiles = range(h * per, (h + 1) * per)
        for n in tiles:
            q[j - 1, n] = summed(j, n).astype(BF16)
        return lambda: [send(j, n).start() for n in tiles]

    def far_total(h):
        d2d_in(3, h)
        fold(jnp.concatenate([summed(3, n) for n in range(h * per, (h + 1) * per)], axis=1), snd2_o, h)
        ret_o[h, 0] = snd2_o[h, 0]
        return lambda: start_all(f_copies[h])

    def down_pass(j):
        down_tiles(j, range(per))
        down_tiles(j, range(per, NT))

    def other_side():
        for h in range(2):
            from_near(2, h)
            pair[2][h].start()

    local[11].wait()
    local[12].wait()
    local[13].wait()
    @pl.when(y != 0)
    def _():
        pair_in(0)
        gate_up(0)

    for is_first, copies in to_near:
        @pl.when(jnp.logical_not(is_first))
        def _():
            copies[0].start()
            copies[1].start()
    from_near(1, 0)
    pair[1][0].start()
    from_near(1, 1)
    pair[1][1].start()
    @pl.when(y != 0)
    def _():
        down_tiles(0, range(NT))

    for h in range(2):
        arrive_all(rcv_o, c_r, h)
        settle(rcv_o, 3, h)
        pair[3][h].start()
    pair_in(1)
    gate_up(1)
    down_pass(1)
    pair_in(3)
    gate_up(3, {2: other_side, 3: lambda: finish(1, 0)})
    down_tiles(3, range(per))
    finish(1, 1)()
    down_tiles(3, range(per, NT))
    pair_in(2)
    gate_up(2)
    down_tiles(2, range(per))
    far_total(0)()
    down_tiles(2, range(per, NT))
    finish(2, 0)()
    far_total(1)()
    finish(2, 1)()

    @pl.when(y == 0)
    def _():
        pair_in(0)
        gate_up(0)
        down_pass(0)

    def picked(place, weight, src, h):
        came = unfold(src, h)
        routed = [
            weight[k] * lax.dot_general(
                place[k].astype(BF16), came, (((0,), (0,)), ((), ())), preferred_element_type=F32
            )
            for k in range(2)
        ]
        return routed[0] + routed[1]

    weight_o = weights(rw_o)
    weight = weights(rw)

    def own_total(h):
        d2d_in(0, h)
        for k in range(2):
            whole(rab.at[k, pl.ds(h * per, per)], q_r.at[2 * k + h])
        sums = [
            summed(0, n) + rab[0, n].astype(F32) + rab[1, n].astype(F32)
            for n in range(h * per, (h + 1) * per)
        ]
        fold(jnp.concatenate(sums, axis=1), snd2, h)
        start_all(e_copies[h])
        ret[h, 0] = snd2[h, 0]

    def far_part(h):
        arrive_all(ret_o, f_r, h)
        part_o[:, h * half:(h + 1) * half] = picked(place_o, weight_o, ret_o, h).astype(BF16)
        far_copies[4 + h].start()

    own_total(0)
    far_part(0)
    own_total(1)
    far_part(1)
    halo_copy.wait_send()

    @pl.when(tp != 0)
    def _():
        remote(term, terms.at[tp], i_s, i_r, (sp, 0)).wait_send()

    for copy in far_copies[:4]:
        copy.wait_send()
    whole(mx.at[pl.ds(1, NTP - 1)], a_s)
    for src, ss in ((snd, b_s), (snd_o, c_s), (snd2_o, f_s)):
        whole(src.at[:, pl.ds(1, NSP - 1)], ss)
    whole(xb.at[0, pl.ds(0, 4 * blk)], g_s)
    whole(xb.at[0], p_s)
    whole(pb, d_s)
    whole(q, q_s)
    for h in range(2):
        cols = slice(h * half, (h + 1) * half)
        arrive_all(ret, e_r, h)
        acc[:, cols] = RESIDUAL * normed[:, cols].astype(F32) + picked(place, weight, ret, h)
    far_copies[4].wait_recv()
    far_copies[5].wait_recv()
    acc[...] += part[...].astype(F32)
    out_ref[...] = layer_norm(acc[...], ng[1:2, :], nb[1:2, :]).astype(BF16)

    far_copies[4].wait_send()
    far_copies[5].wait_send()
    whole(snd2.at[:, pl.ds(1, NSP - 1)], e_s)


def shards(stream, out_gate, in_gate, values, conv_weight, out_weight, doc_ids, routes, route_weight,
           norm_gain, norm_bias, expert_gate, expert_up, expert_down):
    length, width = out_gate.shape
    rows, model = stream.shape
    hidden = expert_gate.shape[2]
    blk = NSP * CAP
    any_spec = pl.BlockSpec(memory_space=pltpu.HBM)
    dma = pltpu.SemaphoreType.DMA
    scratch = [
        pltpu.VMEM((rows, model), BF16),
        pltpu.VMEM((length, width), BF16),
        pltpu.VMEM((length, width), BF16),
        pltpu.VMEM((length, width), BF16),
        pltpu.VMEM((3, width), F32),
        pltpu.VMEM((model, model), BF16),
        pltpu.VMEM((1, length), jnp.int32),
        pltpu.VMEM((2, rows), jnp.int32),
        pltpu.VMEM((2, rows), F32),
        pltpu.VMEM((2, model), F32),
        pltpu.VMEM((2, model), F32),
        pltpu.VMEM((model, hidden), BF16),
        pltpu.VMEM((model, hidden), BF16),
        pltpu.VMEM((hidden, model), BF16),
        pltpu.VMEM((8 + length, width + 128), F32),
        pltpu.VMEM((8, width + 128), F32),
        pltpu.VMEM((2, model), F32),
        pltpu.VMEM((NTP, 2, model), F32),
        pltpu.VMEM((NTP, rows, width), BF16),
        pltpu.VMEM((NTP, rows, width), BF16),
        pltpu.VMEM((rows, model), F32),
        pltpu.VMEM((rows, model), BF16),
        pltpu.VMEM((2, NSP, CAP * LB, 128), BF16),
        pltpu.VMEM((2, NSP, CAP * LB, 128), BF16),
        pltpu.VMEM((2, 8 * blk, model // 2), BF16),
        pltpu.VMEM((2 * blk, hidden), BF16),
        pltpu.VMEM((NT, 4 * blk, model // NT), F32),
        pltpu.VMEM((NT, 4 * blk, model // NT), BF16),
        pltpu.VMEM((NT, 4 * blk, model // NT), BF16),
        pltpu.VMEM((2, NT, blk, model // NT), BF16),
        pltpu.VMEM((2, NT, blk, model // NT), BF16),
        pltpu.VMEM((2, NSP, CAP * LB, 128), BF16),
        pltpu.VMEM((2, NSP, CAP * LB, 128), BF16),
        pltpu.VMEM((2, rows), jnp.int32),
        pltpu.VMEM((2, rows), F32),
        pltpu.VMEM((rows, model), BF16),
        pltpu.VMEM((2, NSP, CAP * LB, 128), BF16),
        pltpu.VMEM((2, NSP, CAP * LB, 128), BF16),
        pltpu.VMEM((2, NSP, CAP * LB, 128), BF16),
        pltpu.VMEM((2, NSP, CAP * LB, 128), BF16),
        pltpu.VMEM((rows, model), BF16),
        pltpu.VMEM((rows, model), BF16),
        pltpu.VMEM((blk * LB, 128), F32),
        dma((14,)), dma, dma, dma, dma, dma, dma((NTP,)), dma, dma((2,)),
        dma, dma((4,)), dma, dma((4,)), dma, dma((8,)),
        dma, dma((4,)), dma, dma((2,)),
        dma((6,)), dma((6,)), dma, dma((2,)), dma, dma((2,)),
    ]
    return pl.pallas_call(
        body,
        out_shape=jax.ShapeDtypeStruct((rows, model), BF16),
        in_specs=[any_spec] * 14,
        out_specs=pl.BlockSpec(memory_space=pltpu.VMEM),
        scratch_shapes=scratch,
        compiler_params=pltpu.CompilerParams(
            collective_id=0, has_side_effects=True, vmem_limit_bytes=48 * 1024 * 1024
        ),
        name="layer",
    )(*[pltpu.with_memory_space_constraint(v, pltpu.HBM) for v in (
        stream, out_gate, in_gate, values, conv_weight, out_weight, doc_ids.reshape(1, -1),
        routes.T, route_weight.T, norm_gain, norm_bias, expert_gate, expert_up, expert_down,
    )])


def solution(mesh):
    in_specs = (
        P(("sp", "tp"), None),
        P("sp", "tp"),
        P("sp", "tp"),
        P("sp", "tp"),
        P(None, "tp"),
        P(),
        P("sp"),
        P(("sp", "tp"), None),
        P(("sp", "tp"), None),
        P(),
        P(),
        P("sp", None, "tp"),
        P("sp", None, "tp"),
        P("sp", "tp", None),
    )
    out_specs = P(("sp", "tp"), None)
    return jax.shard_map(shards, mesh=mesh, in_specs=in_specs, out_specs=out_specs, check_vma=False)
```

```python
import jax
import jax.numpy as jnp
from jax import lax
from jax.experimental import pallas as pl
from jax.experimental.pallas import tpu as pltpu
from jax.sharding import PartitionSpec as P

MESH = pl.DeviceIdType.MESH
RESIDUAL = 1.6817928
NX = 4
NZ = 4
NSP = 16
NTP = 8
CAP = 5
LB = 8
NT = 4
F32 = jnp.float32
BF16 = jnp.bfloat16


def layer_norm(v, gain, bias):
    mean = jnp.mean(v, axis=-1, keepdims=True)
    cent = v - mean
    var = jnp.mean(cent * cent, axis=-1, keepdims=True)
    return cent * lax.rsqrt(var + 1e-05) * gain + bias


def one_hot(cond):
    return jnp.where(cond, 1.0, 0.0).astype(BF16)


def body(
    stream_h, og_h, ig_h, va_h, cw_h, ow_h, doc_h, rt_h, rw_h, ng_h, nb_h, wg_h, wu_h, wd_h,
    out_ref,
    stream, og, ig, va, cw, ow, doc, rt, rw, ng, nb, wg, wu, wd,
    ext, halo, term, terms, mx, tr, acc, normed, snd, rcv, xb, hb, pf, pb, rd, q, rab, snd2, ret,
    rt_o, rw_o, normed_o, snd_o, rcv_o, snd2_o, ret_o, part_o, part, turn,
    lsem, h_s, h_r, i_s, i_r, a_s, a_r, b_s, b_r, g_s, g_r, p_s, p_r, d_s, d_r, q_s, q_r, e_s, e_r,
    o_s, o_r, c_s, c_r, f_s, f_r,
):
    sp = lax.axis_index("sp")
    tp = lax.axis_index("tp")
    z, x = sp // NX, sp % NX
    y, c = tp // 2, tp % 2
    width = og.shape[1]
    length = og.shape[0]
    model = stream.shape[1]
    rows = stream.shape[0]
    hidden = wg.shape[1]
    blk = NSP * CAP
    tile = model // NT
    half = model // 2
    per = NT // 2

    def sp_at(d):
        return ((z + d // NX) % NZ) * NX + (x + d % NX) % NX

    def sp_back(d):
        return ((z - d // NX + NZ) % NZ) * NX + (x - d % NX + NX) % NX

    def tp_at(o):
        return ((y + o // 2) % 4) * 2 + (c + o % 2) % 2

    def tp_from(o):
        return ((y - o // 2 + 4) % 4) * 2 + (c - o % 2 + 2) % 2

    def remote(src, dst, ss, rs, dev):
        return pltpu.make_async_remote_copy(
            src_ref=src, dst_ref=dst, send_sem=ss, recv_sem=rs, device_id=dev, device_id_type=MESH
        )

    def whole(ref, sem):
        remote(ref, ref, sem, sem, (sp, tp)).wait_recv()

    barrier = pltpu.get_barrier_semaphore()
    for d in range(1, NSP):
        pl.semaphore_signal(barrier, inc=1, device_id=(sp_at(d), tp), device_id_type=MESH)
    for o in range(1, NTP):
        pl.semaphore_signal(barrier, inc=1, device_id=(sp, tp_at(o)), device_id_type=MESH)

    nxt = (sp + 1) % NSP

    local = [
        pltpu.make_async_copy(src, dst, lsem.at[i])
        for i, (src, dst) in enumerate(
            [
                (ig_h, ig), (va_h, va), (cw_h, cw), (doc_h, doc), (og_h, og), (rt_h, rt), (rw_h, rw),
                (stream_h, stream), (ng_h, ng), (nb_h, nb), (ow_h, ow),
                (wg_h.at[0], wg), (wu_h.at[0], wu), (wd_h.at[0], wd),
            ]
        )
    ]
    for copy in local[:10]:
        copy.start()

    for i in range(4):
        local[i].wait()
    ext[0:8, :width] = jnp.zeros((8, width), F32)
    ext[0:8, width:] = jnp.full((8, 128), -1.0, F32)
    ext[8:8 + length, :width] = ig[...].astype(F32) * va[...].astype(F32)
    ext[8:8 + length, width:] = jnp.transpose(jnp.broadcast_to(doc[...].astype(F32), (128, length)))
    local[4].wait()
    local[10].start()
    pl.semaphore_wait(barrier, NSP + NTP - 2)
    halo_copy = remote(ext.at[pl.ds(length, 8), :], halo, h_s, h_r, (nxt, tp))
    halo_copy.start()
    far = (sp, ((y + 2) % 4) * 2 + c)
    local[5].wait()
    local[6].wait()
    far_copies = [
        remote(src, dst, o_s.at[i], o_r.at[i], far)
        for i, (src, dst) in enumerate([
            (rt, rt_o), (rw, rw_o),
            (normed.at[:, pl.ds(0, half)], normed_o.at[:, pl.ds(0, half)]),
            (normed.at[:, pl.ds(half, half)], normed_o.at[:, pl.ds(half, half)]),
            (part_o.at[:, pl.ds(0, half)], part.at[:, pl.ds(0, half)]),
            (part_o.at[:, pl.ds(half, half)], part.at[:, pl.ds(half, half)]),
        ])
    ]
    far_copies[0].start()
    far_copies[1].start()

    def convolved(r0, n):
        d0 = ext[8 + r0:8 + r0 + n, width:]
        keep1 = jnp.where(ext[7 + r0:7 + r0 + n, width:] == d0, 1.0, 0.0)
        keep2 = jnp.where(ext[6 + r0:6 + r0 + n, width:] == d0, 1.0, 0.0)
        keep1 = jnp.concatenate([keep1] * (width // 128), axis=1)
        keep2 = jnp.concatenate([keep2] * (width // 128), axis=1)
        return (
            cw[0:1, :] * ext[6 + r0:6 + r0 + n, :width] * keep2
            + cw[1:2, :] * ext[7 + r0:7 + r0 + n, :width] * keep1
            + cw[2:3, :] * ext[8 + r0:8 + r0 + n, :width]
        )

    for t in range(NTP):
        mx[t] = (og[t * rows:(t + 1) * rows, :].astype(F32) * convolved(t * rows, rows)).astype(BF16)
    a_copies = [
        remote(mx.at[tp_at(o)], tr.at[o], a_s, a_r.at[o], (sp, tp_at(o))) for o in range(1, NTP)
    ]
    for o in (4, 5, 2, 3, 6, 7, 1):
        a_copies[o - 1].start()
    for copy in local[11:]:
        copy.start()

    lanes = lax.broadcasted_iota(jnp.int32, (NSP, rows), 0)
    upper = one_hot(
        lax.broadcasted_iota(jnp.int32, (rows, rows), 0) < lax.broadcasted_iota(jnp.int32, (rows, rows), 1)
    )
    slots = lax.broadcasted_iota(jnp.int32, (blk, rows), 0)
    eye = lax.broadcasted_iota(jnp.int32, (rows, rows), 0) == lax.broadcasted_iota(jnp.int32, (rows, rows), 1)

    def placed(table):
        rel = []
        for k in range(2):
            e = table[k:k + 1, :]
            rel.append((((e >> 2) + (NZ - z)) & 3) * NX + (((e & 3) + (NX - x)) & 3))
        hot = [jnp.where(lanes == r, 1.0, 0.0) for r in rel]
        prefix = jnp.dot((hot[0] + hot[1]).astype(BF16), upper, preferred_element_type=F32)
        place = []
        for k in range(2):
            rank = jnp.sum(prefix * hot[k], axis=0, keepdims=True)
            slot = rel[k] * CAP + rank.astype(jnp.int32)
            place.append(jnp.where(slots == slot, 1.0, 0.0))
        return place

    def weights(table):
        return [jnp.sum(jnp.where(eye, table[k:k + 1, :], 0.0), axis=1, keepdims=True) for k in range(2)]

    place = placed(rt)

    for i in range(7, 11):
        local[i].wait()

    def project(lhs, t):
        start = pl.multiple_of(t * width, width)
        return jnp.dot(lhs, ow[pl.ds(start, width), :], preferred_element_type=F32)

    acc[...] = RESIDUAL * stream[...].astype(F32) + project(mx[tp], tp)
    def edge_rows():
        halo_copy.wait_recv()
        ext[0:8, :width] = halo[:, :width]
        ext[0:8, width:] = jnp.where(sp == 0, -1.0, halo[:, width:])
        fixed = (og[0:16, :].astype(F32) * convolved(0, 16)).astype(BF16)
        term[...] = project(fixed, tp)[0:2, :]

        @pl.when(tp != 0)
        def _():
            remote(term, terms.at[tp], i_s, i_r, (sp, 0)).start()

    pl.when(x != 0)(edge_rows)
    for o in (1, 2, 3, 6, 7, 4, 5):
        a_copies[o - 1].wait_recv()
        acc[...] += project(tr[o], tp_from(o))
        if o == 3:
            pl.when(x == 0)(edge_rows)
    @pl.when(tp == 0)
    def _():
        whole(terms.at[pl.ds(1, NTP - 1)], i_r)
        total = term[...]
        for t in range(1, NTP):
            total += terms[t]
        acc[0:2, :] = RESIDUAL * stream[0:2, :].astype(F32) + total

    normed[...] = layer_norm(acc[...], ng[0:1, :], nb[0:1, :]).astype(BF16)

    far_copies[2].start()
    far_copies[3].start()

    def fold(rows_f32, dst, h):
        for b in range(LB):
            turn[pl.ds(b, blk, stride=LB), :] = rows_f32[:, b * 128:(b + 1) * 128]
        dst[h] = turn[...].reshape(NSP, CAP * LB, 128).astype(BF16)

    def unfold(src, h):
        turn[...] = src[h].astype(F32).reshape(blk * LB, 128)
        return jnp.concatenate(
            [turn[pl.ds(b, blk, stride=LB), :].astype(BF16) for b in range(LB)], axis=1
        )

    def pack(place, src, dst, h):
        both = (place[0] + place[1]).astype(BF16)
        fold(jnp.dot(both, src[:, h * half:(h + 1) * half], preferred_element_type=F32), dst, h)

    def halves(src, dst, ss, rs, to):
        return [
            {
                d: remote(src.at[h, d], dst.at[h, d], ss, rs.at[h], (to(d), tp))
                for d in range(1, NSP)
            }
            for h in range(2)
        ]

    sp_order = (10, 9, 11, 6, 14, 5, 7, 13, 15, 2, 8, 1, 3, 4, 12)
    b_copies = halves(snd, rcv, b_s, b_r, sp_at)
    c_copies = halves(snd_o, rcv_o, c_s, c_r, sp_at)
    e_copies = halves(snd2, ret, e_s, e_r, sp_back)
    f_copies = halves(snd2_o, ret_o, f_s, f_r, sp_back)

    def start_all(copies):
        for d in sp_order:
            copies[d].start()

    def arrive_all(dst, rs, h):
        whole(dst.at[h, pl.ds(1, NSP - 1)], rs.at[h])

    for h in range(2):
        pack(place, normed, snd, h)
        start_all(b_copies[h])
        rcv[h, 0] = snd[h, 0]
    far_copies[0].wait_recv()
    far_copies[1].wait_recv()
    place_o = placed(rt_o)
    def side_of(row):
        return (1 - 2 * c) * (2 * (((row + 1) % 4) // 2) - 1)

    side = side_of(y)
    above, below = (y + 1) % 4, (y + 3) % 4
    first_above = side_of(above) == -1
    first_below = side_of(below) == 1
    toward = [(sp, ((y + side + 4) % 4) * 2 + c), (sp, ((y - side + 4) % 4) * 2 + c)]
    mate = (sp, y * 2 + 1 - c)
    position = {0: 0, 4: 1, 3: 2, 7: 3, 1: 4, 5: 5, 2: 6, 6: 7}

    def settle(src, j, h):
        r0 = position[j] * blk
        xb[h, r0:r0 + blk, :] = unfold(src, h)

    def block(j, h):
        return xb.at[h, pl.ds(position[j] * blk, blk), :]

    def neighbour(row, is_first, h):
        k = jnp.where(is_first, 0, 1)
        rows_at = pl.multiple_of((position[1] + k * (position[2] - position[1])) * blk, blk)
        return remote(
            block(0, h), xb.at[h, pl.ds(rows_at, blk), :], g_s, g_r.at[2 * k + h], (sp, row * 2 + c)
        )

    to_near = [
        (first_above, [neighbour(above, first_above, h) for h in range(2)]),
        (first_below, [neighbour(below, first_below, h) for h in range(2)]),
    ]

    def from_near(j, h):
        remote(block(0, h), block(j, h), g_s, g_r.at[2 * (j - 1) + h], mate).wait_recv()

    pair = [
        [remote(block(j, h), block(4 + j, h), p_s, p_r.at[j], mate) for h in range(2)]
        for j in range(4)
    ]

    def gather_half(h):
        arrive_all(rcv, b_r, h)
        settle(rcv, 0, h)
        pair[0][h].start()
        for is_first, copies in to_near:
            @pl.when(is_first)
            def _():
                copies[h].start()

    def far_dispatch():
        for h in range(2):
            far_copies[2 + h].wait_recv()
            pack(place_o, normed_o, snd_o, h)
            start_all(c_copies[h])
            rcv_o[h, 0] = snd_o[h, 0]

    pl.when(tp == 0)(far_dispatch)
    gather_half(0)
    pl.when((tp != 0) & (tp != 4))(far_dispatch)
    gather_half(1)
    pl.when(tp == 4)(far_dispatch)

    def gate_up(j, beside={}):
        r0 = position[j] * blk
        lo, hi = (xb.at[h, pl.ds(r0, 2 * blk), :] for h in range(2))
        for i, c0 in enumerate(range(0, hidden, 256)):
            cols = slice(c0, min(c0 + 256, hidden))
            start = beside[i]() if i in beside else None
            gate, upp = [
                jnp.dot(lo[...], w[:half, cols], preferred_element_type=F32)
                + jnp.dot(hi[...], w[half:, cols], preferred_element_type=F32)
                for w in (wg, wu)
            ]
            hb[:, cols] = (gate / (1.0 + jnp.exp(-gate)) * upp).astype(BF16)
            if start:
                start()

    def d2d(j, n):
        view = (n, pl.ds(j * blk, blk))
        return remote(pb.at[view], rd.at[view], d_s, d_r.at[2 * j + n // per], mate)

    def d2d_in(j, h):
        whole(rd.at[pl.ds(h * per, per), pl.ds(j * blk, blk)], d_r.at[2 * j + h])

    def pair_in(j):
        whole(xb.at[:, pl.ds(position[4 + j] * blk, blk)], p_r.at[j])

    def down_tiles(j, tiles):
        for n in tiles:
            part = jnp.dot(hb[...], wd[:, n * tile:(n + 1) * tile], preferred_element_type=F32)
            pf[n, j * blk:(j + 1) * blk, :] = part[:blk]
            pb[n, j * blk:(j + 1) * blk, :] = part[blk:].astype(BF16)
        for n in tiles:
            d2d(j, n).start()

    behind = (1 + side) // 2

    def send(j, n):
        k = behind if j == 1 else 1 - behind
        return remote(q.at[j - 1, n], rab.at[k, n], q_s, q_r.at[2 * k + n // per], toward[j - 1])

    def summed(j, n):
        return pf[n, j * blk:(j + 1) * blk, :] + rd[n, j * blk:(j + 1) * blk, :].astype(F32)

    def finish(j, h):
        d2d_in(j, h)
        tiles = range(h * per, (h + 1) * per)
        for n in tiles:
            q[j - 1, n] = summed(j, n).astype(BF16)
        return lambda: [send(j, n).start() for n in tiles]

    def far_total(h):
        d2d_in(3, h)
        fold(jnp.concatenate([summed(3, n) for n in range(h * per, (h + 1) * per)], axis=1), snd2_o, h)
        ret_o[h, 0] = snd2_o[h, 0]
        return lambda: start_all(f_copies[h])

    def down_pass(j):
        down_tiles(j, range(per))
        down_tiles(j, range(per, NT))

    def other_side():
        for h in range(2):
            from_near(2, h)
            pair[2][h].start()

    local[11].wait()
    local[12].wait()
    local[13].wait()
    @pl.when(y != 0)
    def _():
        pair_in(0)
        gate_up(0)

    for is_first, copies in to_near:
        @pl.when(jnp.logical_not(is_first))
        def _():
            copies[0].start()
            copies[1].start()
    from_near(1, 0)
    pair[1][0].start()
    @pl.when(y != 0)
    def _():
        down_tiles(0, range(NT))

    from_near(1, 1)
    pair[1][1].start()
    for h in range(2):
        arrive_all(rcv_o, c_r, h)
        settle(rcv_o, 3, h)
        pair[3][h].start()
    pair_in(1)
    gate_up(1)
    down_pass(1)
    pair_in(3)
    gate_up(3, {2: other_side, 3: lambda: finish(1, 0)})
    down_tiles(3, range(per))
    finish(1, 1)()
    down_tiles(3, range(per, NT))
    pair_in(2)
    gate_up(2)
    down_tiles(2, range(per))
    far_total(0)()
    down_tiles(2, range(per, NT))
    finish(2, 0)()
    far_total(1)()
    finish(2, 1)()

    @pl.when(y == 0)
    def _():
        pair_in(0)
        gate_up(0)
        down_pass(0)

    def picked(place, weight, src, h):
        came = unfold(src, h)
        routed = [
            weight[k] * lax.dot_general(
                place[k].astype(BF16), came, (((0,), (0,)), ((), ())), preferred_element_type=F32
            )
            for k in range(2)
        ]
        return routed[0] + routed[1]

    weight_o = weights(rw_o)
    weight = weights(rw)

    def own_total(h):
        d2d_in(0, h)
        for k in range(2):
            whole(rab.at[k, pl.ds(h * per, per)], q_r.at[2 * k + h])
        sums = [
            summed(0, n) + rab[0, n].astype(F32) + rab[1, n].astype(F32)
            for n in range(h * per, (h + 1) * per)
        ]
        fold(jnp.concatenate(sums, axis=1), snd2, h)
        start_all(e_copies[h])
        ret[h, 0] = snd2[h, 0]

    def far_part(h):
        arrive_all(ret_o, f_r, h)
        part_o[:, h * half:(h + 1) * half] = picked(place_o, weight_o, ret_o, h).astype(BF16)
        far_copies[4 + h].start()

    own_total(0)
    far_part(0)
    own_total(1)
    far_part(1)
    halo_copy.wait_send()

    @pl.when(tp != 0)
    def _():
        remote(term, terms.at[tp], i_s, i_r, (sp, 0)).wait_send()

    for copy in far_copies[:4]:
        copy.wait_send()
    whole(mx.at[pl.ds(1, NTP - 1)], a_s)
    for src, ss in ((snd, b_s), (snd_o, c_s), (snd2_o, f_s)):
        whole(src.at[:, pl.ds(1, NSP - 1)], ss)
    whole(xb.at[0, pl.ds(0, 4 * blk)], g_s)
    whole(xb.at[0], p_s)
    whole(pb, d_s)
    whole(q, q_s)
    for h in range(2):
        cols = slice(h * half, (h + 1) * half)
        arrive_all(ret, e_r, h)
        acc[:, cols] = RESIDUAL * normed[:, cols].astype(F32) + picked(place, weight, ret, h)
    far_copies[4].wait_recv()
    far_copies[5].wait_recv()
    acc[...] += part[...].astype(F32)
    out_ref[...] = layer_norm(acc[...], ng[1:2, :], nb[1:2, :]).astype(BF16)

    far_copies[4].wait_send()
    far_copies[5].wait_send()
    whole(snd2.at[:, pl.ds(1, NSP - 1)], e_s)


def shards(stream, out_gate, in_gate, values, conv_weight, out_weight, doc_ids, routes, route_weight,
           norm_gain, norm_bias, expert_gate, expert_up, expert_down):
    length, width = out_gate.shape
    rows, model = stream.shape
    hidden = expert_gate.shape[2]
    blk = NSP * CAP
    any_spec = pl.BlockSpec(memory_space=pltpu.HBM)
    dma = pltpu.SemaphoreType.DMA
    scratch = [
        pltpu.VMEM((rows, model), BF16),
        pltpu.VMEM((length, width), BF16),
        pltpu.VMEM((length, width), BF16),
        pltpu.VMEM((length, width), BF16),
        pltpu.VMEM((3, width), F32),
        pltpu.VMEM((model, model), BF16),
        pltpu.VMEM((1, length), jnp.int32),
        pltpu.VMEM((2, rows), jnp.int32),
        pltpu.VMEM((2, rows), F32),
        pltpu.VMEM((2, model), F32),
        pltpu.VMEM((2, model), F32),
        pltpu.VMEM((model, hidden), BF16),
        pltpu.VMEM((model, hidden), BF16),
        pltpu.VMEM((hidden, model), BF16),
        pltpu.VMEM((8 + length, width + 128), F32),
        pltpu.VMEM((8, width + 128), F32),
        pltpu.VMEM((2, model), F32),
        pltpu.VMEM((NTP, 2, model), F32),
        pltpu.VMEM((NTP, rows, width), BF16),
        pltpu.VMEM((NTP, rows, width), BF16),
        pltpu.VMEM((rows, model), F32),
        pltpu.VMEM((rows, model), BF16),
        pltpu.VMEM((2, NSP, CAP * LB, 128), BF16),
        pltpu.VMEM((2, NSP, CAP * LB, 128), BF16),
        pltpu.VMEM((2, 8 * blk, model // 2), BF16),
        pltpu.VMEM((2 * blk, hidden), BF16),
        pltpu.VMEM((NT, 4 * blk, model // NT), F32),
        pltpu.VMEM((NT, 4 * blk, model // NT), BF16),
        pltpu.VMEM((NT, 4 * blk, model // NT), BF16),
        pltpu.VMEM((2, NT, blk, model // NT), BF16),
        pltpu.VMEM((2, NT, blk, model // NT), BF16),
        pltpu.VMEM((2, NSP, CAP * LB, 128), BF16),
        pltpu.VMEM((2, NSP, CAP * LB, 128), BF16),
        pltpu.VMEM((2, rows), jnp.int32),
        pltpu.VMEM((2, rows), F32),
        pltpu.VMEM((rows, model), BF16),
        pltpu.VMEM((2, NSP, CAP * LB, 128), BF16),
        pltpu.VMEM((2, NSP, CAP * LB, 128), BF16),
        pltpu.VMEM((2, NSP, CAP * LB, 128), BF16),
        pltpu.VMEM((2, NSP, CAP * LB, 128), BF16),
        pltpu.VMEM((rows, model), BF16),
        pltpu.VMEM((rows, model), BF16),
        pltpu.VMEM((blk * LB, 128), F32),
        dma((14,)), dma, dma, dma, dma, dma, dma((NTP,)), dma, dma((2,)),
        dma, dma((4,)), dma, dma((4,)), dma, dma((8,)),
        dma, dma((4,)), dma, dma((2,)),
        dma((6,)), dma((6,)), dma, dma((2,)), dma, dma((2,)),
    ]
    return pl.pallas_call(
        body,
        out_shape=jax.ShapeDtypeStruct((rows, model), BF16),
        in_specs=[any_spec] * 14,
        out_specs=pl.BlockSpec(memory_space=pltpu.VMEM),
        scratch_shapes=scratch,
        compiler_params=pltpu.CompilerParams(
            collective_id=0, has_side_effects=True, vmem_limit_bytes=48 * 1024 * 1024
        ),
        name="layer",
    )(*[pltpu.with_memory_space_constraint(v, pltpu.HBM) for v in (
        stream, out_gate, in_gate, values, conv_weight, out_weight, doc_ids.reshape(1, -1),
        routes.T, route_weight.T, norm_gain, norm_bias, expert_gate, expert_up, expert_down,
    )])


def solution(mesh):
    in_specs = (
        P(("sp", "tp"), None),
        P("sp", "tp"),
        P("sp", "tp"),
        P("sp", "tp"),
        P(None, "tp"),
        P(),
        P("sp"),
        P(("sp", "tp"), None),
        P(("sp", "tp"), None),
        P(),
        P(),
        P("sp", None, "tp"),
        P("sp", None, "tp"),
        P("sp", "tp", None),
    )
    out_specs = P(("sp", "tp"), None)
    return jax.shard_map(shards, mesh=mesh, in_specs=in_specs, out_specs=out_specs, check_vma=False)
```
